256 devices in a mesh: sp: 32 (over z, y), tp: 8 (over x, core).
Axes of the slice: x: 4, y: 4, z: 8, core: 2. Of those that a mesh axis runs over, the one named last changes fastest.
Arguments:
- queries: bfloat16 [32768, 1024], P('sp', 'tp'), may hold values from -6 to 6
- cell_key_rows: bfloat16 [32768, 1024], P('sp', 'tp'), may hold values from -6 to 6
- cell_value_rows: bfloat16 [32768, 2048], P('sp', 'tp'), may hold values from -6 to 6
- output_gate_logits: bfloat16 [32768, 2048], P('sp', 'tp'), may hold values from -6 to 6
- input_gate_logits: bfloat16 [8, 32768], P('tp', 'sp'), may hold values from -4 to 216
- forget_gate_logits: bfloat16 [8, 32768], P('tp', 'sp'), may hold values from 0.5 to 14
- forget_extra_term: float32 [8, 32768], P('tp', 'sp'), may hold values from -1.4 to 0
- residual: bfloat16 [32768, 2048], P('sp', 'tp'), may hold values from -13 to 13
- head_norm_gain: bfloat16 [2048], P('tp'), may hold values from 0.099609375 to 1.8984375
- cell_output_weight: bfloat16 [2048, 2048], P('tp'), may hold values from -0.25 to 0.25
- feedforward_norm_gain: bfloat16 [2048], replicated, may hold values from 0.099609375 to 1.8984375
- gate_projection_weight: bfloat16 [2048, 5632], P('sp', 'tp'), may hold values from -0.125 to 0.125
- up_projection_weight: bfloat16 [2048, 5632], P('sp', 'tp'), may hold values from -0.125 to 0.125
- down_projection_weight: bfloat16 [5632, 2048], P('tp', 'sp'), may hold values from -0.15625 to 0.15625
Outputs:
- mixed: bfloat16 [32768, 2048], P('sp', 'tp')
The draws below stay inside these ranges and needn't reach their ends.
All inputs are finite; a program needn't handle non-finite values.
Results may differ from the reference program's by a relative error of at most 0.017.
Values may be sent and summed in bfloat16 or wider, within the bound.
No kernel may reach another device: no remote copies, remote signals or barrier semaphores. Data moves between devices by JAX's collectives and lax.ppermute only.
A program may use at most 64 MiB of HBM per device.

```python
import jax
import jax.numpy as jnp
from jax import lax

D = 2048
HEADS = 8
DK = 128
DV = 256
FF = 5632
TOK_DEV = 1024
TOKENS = 32768
N_TP = 8


def draw_input_gate_logits(key, part):
    base_key = jax.random.fold_in(key, 11)
    values = jnp.clip(jax.random.normal(base_key, (HEADS, TOKENS), jnp.float32), -4.0, 4.0)
    return values.astype(jnp.bfloat16)


def draw_forget_gate_logits(key, part):
    order = jax.random.permutation(jax.random.fold_in(key, 21), HEADS)
    noise_key = jax.random.fold_in(key, 22)
    slow_count = HEADS // 2
    jitter = 0.6 * jnp.clip(jax.random.normal(noise_key, (HEADS, TOKENS), jnp.float32), -4.0, 4.0)
    slow_heads = order < slow_count
    quick = jnp.log(jax.random.uniform(jax.random.fold_in(key, 23), (HEADS,), jnp.float32, 30.0, 60.0))
    level = jnp.where(slow_heads, jnp.log(TOKENS / 0.8), quick)
    block_shift = jax.random.uniform(jax.random.fold_in(key, 24), (HEADS, TOKENS // TOK_DEV), jnp.float32, -0.4, 0.4)
    shifts = jnp.repeat(block_shift, TOK_DEV, axis=1)
    return (level[:, None] + shifts + jitter).astype(jnp.bfloat16)


def draw_forget_extra_term(key, part):
    spots = jax.random.randint(jax.random.fold_in(key, 31), (HEADS, 2, 1), 0, TOKENS)
    fraction = jax.random.uniform(jax.random.fold_in(key, 32), (HEADS, 2, 1), jnp.float32, 0.2, 0.5)
    depth = jnp.log(1.0 - fraction)
    places = jnp.arange(TOKENS)[None, None, :]
    return jnp.sum(jnp.where(places == spots, depth, 0.0), axis=1).astype(jnp.float32)


def draw_residual(key, part):
    column_scale = 0.4 * 6.0 ** (jnp.arange(D, dtype=jnp.float32) / D)
    values = jnp.clip(jax.random.normal(jax.random.fold_in(key, 41), (TOKENS, D), jnp.float32), -4.0, 4.0)
    return (values * column_scale[None, :]).astype(jnp.bfloat16)


def block_levels(rng, dims, shards, low, largest):
    factor_of, own = 1.0, jax.random.fold_in(rng, 6)
    for position, parts in shards:
        steps = jnp.exp(jax.random.uniform(jax.random.fold_in(own, position), (parts,), jnp.float32, low / len(shards), largest / len(shards)))
        factor_of = factor_of * jnp.repeat(steps, dims[position] // parts).reshape([-1 if axis == position else 1 for axis in range(len(dims))])
    return factor_of


def normal_values(rng, shape, spread, most, split=(), held_as=jnp.bfloat16):
    loudness = block_levels(rng, shape, split, -0.22, 0.18) if split else 1.0
    result = jax.random.normal(rng, shape, jnp.float32) * spread * loudness
    return jnp.minimum(jnp.maximum(result, -most), most).astype(held_as)


def setup_inputs(seed: int = 0) -> dict:
    arg_keys = jax.random.split(jax.random.key(seed), 15)
    return {
        "queries": normal_values(arg_keys[0], (TOKENS, HEADS * DK), 1.0, 6.0, ((0, 32), (1, 8))),
        "cell_key_rows": normal_values(arg_keys[1], (TOKENS, HEADS * DK), 1.0, 6.0, ((0, 32), (1, 8))),
        "cell_value_rows": normal_values(arg_keys[2], (TOKENS, HEADS * DV), 1.0, 6.0, ((0, 32), (1, 8))),
        "output_gate_logits": normal_values(arg_keys[3], (TOKENS, HEADS * DV), 1.0, 6.0, ((0, 32), (1, 8))),
        "input_gate_logits": draw_input_gate_logits(jax.random.fold_in(arg_keys[14], 71), 0),
        "forget_gate_logits": draw_forget_gate_logits(jax.random.fold_in(arg_keys[14], 71), 0),
        "forget_extra_term": draw_forget_extra_term(jax.random.fold_in(arg_keys[14], 71), 0),
        "residual": draw_residual(jax.random.fold_in(arg_keys[14], 71), 0),
        "head_norm_gain": jnp.clip(1.0 + 0.18 * jax.random.normal(arg_keys[8], (HEADS * DV,), jnp.float32), 0.099609375, 1.8984375).astype(jnp.bfloat16),
        "cell_output_weight": normal_values(arg_keys[9], (HEADS * DV, D), (HEADS * DV // 4) ** -0.5, 0.25, ((0, 8),)),
        "feedforward_norm_gain": jnp.clip(1.0 + 0.18 * jax.random.normal(arg_keys[10], (D,), jnp.float32), 0.099609375, 1.8984375).astype(jnp.bfloat16),
        "gate_projection_weight": normal_values(arg_keys[11], (D, FF), D ** -0.5, 0.125, ((0, 32), (1, 8))),
        "up_projection_weight": normal_values(arg_keys[12], (D, FF), D ** -0.5, 0.125, ((0, 32), (1, 8))),
        "down_projection_weight": normal_values(arg_keys[13], (FF, D), (FF // 4) ** -0.5, 0.15625, ((0, 8), (1, 32))),
    }


PRECISE = lax.Precision.HIGHEST
LOWEST_LOG = -1e+30
EPSILON = 1e-06

def to_blocks(array, block_count, block_size):
    shaped = array.reshape((array.shape[0], block_count, block_size) + array.shape[2:])
    return jnp.moveaxis(shaped, 1, 0)

def from_blocks(array):
    moved = jnp.moveaxis(array, 0, 1)
    return moved.reshape((moved.shape[0], moved.shape[1] * moved.shape[2]) + moved.shape[3:])

def memory_blocks(query_heads, key_heads, value_heads, in_gates, forget_log_value, block_size):
    head_count, length, key_width = query_heads.shape
    value_width = value_heads.shape[2]
    block_count = length // block_size
    causal = jnp.tril(jnp.ones((block_size, block_size), bool))

    def advance(carried, pieces):
        memory_state, top_log, offset = carried
        query_block, key_block, value_block, gate_block, forget_block = pieces
        running = jnp.cumsum(forget_block, axis=-1)
        log_weight = jnp.where(causal, running[:, :, None] - running[:, None, :] + gate_block[:, None, :], -jnp.inf)
        log_start = running + top_log[:, None]
        row_max = jnp.maximum(lax.optimization_barrier(jnp.max(log_weight, axis=-1)), log_start)
        scores = jnp.einsum('htd,hsd->hts', query_block, key_block, precision=PRECISE)
        scores = scores * jnp.exp(log_weight - row_max[:, :, None])
        earlier = jnp.einsum('htd,hde->hte', query_block, memory_state, precision=PRECISE)
        numerator = jnp.exp(log_start - row_max)[:, :, None] * earlier
        numerator = numerator + jnp.einsum('hts,hse->hte', scores, value_block, precision=PRECISE)
        last_cum = running[:, -1]
        log_end = last_cum[:, None] - running + gate_block
        new_top = jnp.maximum(last_cum + top_log, lax.optimization_barrier(jnp.max(log_end, axis=-1)))
        scaled = key_block * jnp.exp(log_end - new_top[:, None])[:, :, None]
        memory_state = jnp.exp(last_cum + top_log - new_top)[:, None, None] * memory_state
        memory_state = memory_state + jnp.einsum('hsd,hse->hde', scaled, value_block, precision=PRECISE)
        return ((memory_state, new_top, offset + last_cum), (numerator, row_max, offset[:, None] + running))
    initial = (jnp.zeros((head_count, key_width, value_width), jnp.float32), jnp.full((head_count,), LOWEST_LOG, jnp.float32), jnp.zeros((head_count,), jnp.float32))
    pieces = tuple((to_blocks(array, block_count, block_size) for array in (query_heads, key_heads, value_heads, in_gates, forget_log_value)))
    ending, outputs = lax.scan(advance, initial, pieces)
    return (tuple((from_blocks(output) for output in outputs)), ending)

def reference(queries, cell_key_rows, cell_value_rows, output_gate_logits, input_gate_logits, forget_gate_logits, forget_extra_term, residual, head_norm_gain, cell_output_weight, feedforward_norm_gain, gate_projection_weight, up_projection_weight, down_projection_weight):
    length = queries.shape[0]

    def heads_first(array, width):
        return jnp.transpose(array.reshape(length, HEADS, width), (1, 0, 2)).astype(jnp.float32)
    query_heads = heads_first(queries, DK) * DK ** (-0.5)
    key_heads = heads_first(cell_key_rows, DK)
    value_heads = heads_first(cell_value_rows, DV)
    forget_log_value = jax.nn.log_sigmoid(forget_gate_logits.astype(jnp.float32)) + forget_extra_term
    results, _ = memory_blocks(query_heads, key_heads, value_heads, input_gate_logits.astype(jnp.float32), forget_log_value, min(length, 256))
    memory = jnp.transpose(results[0], (1, 0, 2))
    normal = memory * lax.rsqrt(lax.optimization_barrier(jnp.mean(memory * memory, axis=-1, keepdims=True)) + EPSILON)
    gate_open = jax.nn.sigmoid(output_gate_logits.astype(jnp.float32).reshape(length, HEADS, DV))
    gated_heads = normal * head_norm_gain.astype(jnp.float32).reshape(HEADS, DV) * gate_open
    gated_heads = gated_heads.reshape(length, HEADS * DV).astype(jnp.bfloat16)
    head_width = HEADS * DV // N_TP
    stream_sum = residual.astype(jnp.float32)
    for head_part in range(N_TP):
        head_lower = head_part * head_width
        head_term = jnp.dot(gated_heads[:, head_lower:head_lower + head_width], cell_output_weight[head_lower:head_lower + head_width], preferred_element_type=jnp.float32)
        head_rounded = lax.optimization_barrier(head_term.astype(jnp.bfloat16))
        stream_sum = stream_sum + head_rounded.astype(jnp.float32)
    stream = stream_sum.astype(jnp.bfloat16)
    stream_wide = stream.astype(jnp.float32)
    scale = lax.rsqrt(lax.optimization_barrier(jnp.mean(stream_wide * stream_wide, axis=-1, keepdims=True)) + EPSILON)
    normed = (stream_wide * scale * feedforward_norm_gain.astype(jnp.float32)).astype(jnp.bfloat16)
    gate_value = jnp.dot(normed, gate_projection_weight, preferred_element_type=jnp.float32)
    lifted = jnp.dot(normed, up_projection_weight, preferred_element_type=jnp.float32)
    hidden = (jax.nn.silu(gate_value) * lifted).astype(jnp.bfloat16)
    part_width = FF // N_TP
    summed = jnp.zeros(stream_wide.shape, jnp.float32)
    for part_index in range(N_TP):
        lower = part_index * part_width
        partial_value = jnp.dot(hidden[:, lower:lower + part_width], down_projection_weight[lower:lower + part_width], preferred_element_type=jnp.float32)
        rounded = lax.optimization_barrier(partial_value.astype(jnp.bfloat16))
        summed = summed + rounded.astype(jnp.float32)
    return (stream_wide + 0.5 * summed).astype(jnp.bfloat16)
```

```python
import functools

import jax
import jax.numpy as jnp
from jax import lax
from jax.experimental import pallas as pl
from jax.experimental.pallas import tpu as pltpu
from jax.sharding import Mesh
from jax.sharding import PartitionSpec as P

SP = ("z", "y")
TP = ("x", "c")
BF = jnp.bfloat16
F32 = jnp.float32
LOWEST = -1e30
EPSILON = 1e-06
ROWS = 1024
HALF = 512
DK = 128
DV = 256
MSG = 144
FFD = 704

VMEM = pl.BlockSpec(memory_space=pltpu.VMEM)
SMEM = pl.BlockSpec(memory_space=pltpu.SMEM)
ANY = pl.BlockSpec(memory_space=pl.ANY)


def call(body, outs, ins, scratch=(), flops=1000000, in_specs=None, name=None):
    return pl.pallas_call(
        body,
        out_shape=outs,
        in_specs=in_specs or [VMEM] * len(ins),
        out_specs=jax.tree.map(lambda _: VMEM, outs),
        scratch_shapes=list(scratch),
        name=name,
        cost_estimate=pl.CostEstimate(flops=flops, bytes_accessed=1000000, transcendentals=0),
        compiler_params=pltpu.CompilerParams(vmem_limit_bytes=60 * 1024 * 1024),
    )(*ins)


def shape(dims, dtype=BF):
    return jax.ShapeDtypeStruct(dims, dtype)


def scan_rows(values, combine, fill):
    lane = lax.broadcasted_iota(jnp.int32, (8, 128), 1)
    row = lax.broadcasted_iota(jnp.int32, (8, 128), 0)
    for step in (1, 2, 4, 8, 16, 32, 64):
        moved = pltpu.roll(values, step, 1)
        values = combine(values, jnp.where(lane >= step, moved, fill))
    last = jnp.broadcast_to(values[:, 127:128], (8, 128))
    before = jnp.where(row >= 1, pltpu.roll(last, 1, 0), fill)
    for step in (1, 2, 4):
        moved = pltpu.roll(before, step, 0)
        before = combine(before, jnp.where(row >= step, moved, fill))
    return combine(values, before)


def eight_rows(ref):
    wide = ref[...].astype(F32)
    return jnp.concatenate([wide[:, 128 * k : 128 * (k + 1)] for k in range(8)], axis=0)


def as_column(values, k):
    return jnp.transpose(jnp.broadcast_to(values[k : k + 1, :], (128, 128)))


def split3(value):
    high = value.astype(BF).astype(F32)
    middle = (value - high).astype(BF).astype(F32)
    return high, middle, value - high - middle


def scalar_tile(top, total, width=256):
    row = lax.broadcasted_iota(jnp.int32, (16, width), 0)
    tile = jnp.zeros((16, width), F32)
    for k, part in enumerate(split3(top) + split3(total)):
        tile = jnp.where(row == k, jnp.broadcast_to(part, (16, width)), tile)
    return tile.astype(BF)


def read_message(ref):
    tile = ref[DK:MSG, :].astype(F32)
    top = tile[0:1] + tile[1:2] + tile[2:3]
    total = tile[3:4] + tile[4:5] + tile[5:6]
    return ref[0:DK, :].astype(F32), top, total


def summary_body(k_ref, v_ref, ig_ref, fg_ref, fe_ref, msg_ref, a_ref):
    gate = eight_rows(ig_ref)
    forget = eight_rows(fg_ref)
    extra = eight_rows(fe_ref)
    small = jnp.exp(-jnp.abs(forget))
    series = small * (1.0 - small * (0.5 - small * (1 / 3 - small * (0.25 - small * 0.2))))
    log_one = jnp.where(small < 0.03, series, jnp.log(1.0 + small))
    log_forget = jnp.minimum(forget, 0.0) - log_one + extra
    running = scan_rows(log_forget, jnp.add, 0.0)
    level = gate - running
    highest = scan_rows(level, jnp.maximum, LOWEST)
    a_ref[0] = level
    a_ref[1] = highest
    final = jnp.broadcast_to(highest[7:8, 127:128], (8, 128))
    weight = jnp.exp(level - final)
    total = jnp.zeros((DK, DV), F32)
    for b in range(8):
        rows = slice(128 * b, 128 * (b + 1))
        scaled = (k_ref[rows, :].astype(F32) * as_column(weight, b)).astype(BF)
        total = total + lax.dot_general(
            scaled, v_ref[rows, :], (((0,), (0,)), ((), ())), preferred_element_type=F32
        )
    msg_ref[0:DK, :] = total.astype(BF)
    all_forget = running[7:8, 127:128]
    msg_ref[DK:MSG, :] = scalar_tile(highest[7:8, 127:128] + all_forget, all_forget)


def inside_body(q_ref, k_ref, v_ref, a_ref, num_ref):
    level = a_ref[0]
    highest = a_ref[1]
    t = lax.broadcasted_iota(jnp.int32, (256, 256), 0)
    s = lax.broadcasted_iota(jnp.int32, (256, 256), 1)
    causal = t >= s
    for i in range(4):
        left = jnp.concatenate([as_column(highest, 2 * i), as_column(highest, 2 * i + 1)], axis=0)
        column = jnp.concatenate([left, left], axis=1)
        query = q_ref[256 * i : 256 * (i + 1), :]
        total = jnp.zeros((256, DV), F32)
        for j in range(i + 1):
            rows = slice(256 * j, 256 * (j + 1))
            line = jnp.concatenate([level[2 * j : 2 * j + 1], level[2 * j + 1 : 2 * j + 2]], axis=1)
            score = lax.dot_general(
                query, k_ref[rows, :], (((1,), (1,)), ((), ())), preferred_element_type=F32
            )
            weight = jnp.exp(line - column)
            if i == j:
                weight = jnp.where(causal, weight, 0.0)
            total = total + jnp.dot(
                (score * weight).astype(BF), v_ref[rows, :], preferred_element_type=F32
            )
        num_ref[256 * i : 256 * (i + 1), :] = total


def plane_body(id_ref, m0, m1, m2, m3, plane_ref, prefix_ref):
    y = id_ref[1]
    parts = [read_message(m) for m in (m0, m1, m2, m3)]
    place = [lax.rem(y - r + 4, 4) for r in range(4)]
    levels, befores = [], []
    total_all = jnp.zeros((1, DV), F32)
    total_before = jnp.zeros((1, DV), F32)
    for r in range(4):
        level = parts[r][1]
        before = parts[r][1]
        for w in range(4):
            if w != r:
                later = place[w] > place[r]
                level = level + jnp.where(later, parts[w][2], 0.0)
                before = before + jnp.where(later & (place[w] < y), parts[w][2], 0.0)
        levels.append(level)
        befores.append(jnp.where(place[r] < y, before, LOWEST))
        total_all = total_all + parts[r][2]
        total_before = total_before + jnp.where(place[r] < y, parts[r][2], 0.0)
    top = functools.reduce(jnp.maximum, levels)
    top_before = functools.reduce(jnp.maximum, befores)
    whole = jnp.zeros((DK, DV), F32)
    early = jnp.zeros((DK, DV), F32)
    for r in range(4):
        whole = whole + jnp.exp(levels[r] - top) * parts[r][0]
        share = jnp.where(place[r] < y, jnp.exp(befores[r] - top_before), 0.0)
        early = early + share * parts[r][0]
    plane_ref[0:DK, :] = whole.astype(BF)
    plane_ref[DK:MSG, :] = scalar_tile(top, total_all)
    prefix_ref[0:DK, :] = early
    prefix_ref[DK : DK + 8, :] = jnp.broadcast_to(top_before, (8, DV))
    prefix_ref[DK + 8 : DK + 16, :] = jnp.broadcast_to(total_before, (8, DV))


def gated_body(
    id_ref, m1, m2, m3, m4, m5, m6, m7, prefix_ref, num_ref, q_ref, a_ref, o_ref, gain_ref,
    keep_ref, send_ref,
):
    z = id_ref[0]
    c = id_ref[3]
    top_before = prefix_ref[DK : DK + 1, :]
    moved = prefix_ref[DK + 8 : DK + 9, :]
    levels = []
    states = []
    for r, m in enumerate((m1, m2, m3, m4, m5, m6, m7)):
        state, top, total = read_message(m)
        levels.append(jnp.where(z > r, top + moved, LOWEST))
        moved = moved + jnp.where(z > r, total, 0.0)
        states.append(state)
    top = functools.reduce(jnp.maximum, levels, top_before)
    carried = jnp.exp(top_before - top) * prefix_ref[0:DK, :]
    for r in range(7):
        share = jnp.where(z > r, jnp.exp(levels[r] - top), 0.0)
        carried = carried + share * states[r]
    high = carried.astype(BF)
    highest = a_ref[1]
    gain = gain_ref[...].astype(F32)
    for side, out in ((1 - c, send_ref), (c, keep_ref)):
        half = jnp.where(side == 0, highest[0:4], highest[4:8])
        for b in range(2):
            begin = pl.multiple_of(side * HALF + 256 * b, 256)
            rows = pl.ds(begin, 256)
            left = jnp.concatenate([as_column(half, 2 * b), as_column(half, 2 * b + 1)], axis=0)
            inner = jnp.concatenate([left, left], axis=1)
            row_max = jnp.maximum(inner, top)
            outer = jnp.dot(q_ref[rows, :], high, preferred_element_type=F32)
            memory = jnp.exp(inner - row_max) * num_ref[rows, :] + jnp.exp(top - row_max) * outer
            memory = memory * (DK**-0.5)
            mean = jnp.sum(memory * memory, axis=1, keepdims=True) * (1.0 / DV)
            normal = memory * lax.rsqrt(mean + EPSILON)
            opened = jax.nn.sigmoid(o_ref[rows, :].astype(F32))
            out[256 * b : 256 * (b + 1), :] = (normal * gain * opened).astype(BF)


def stream_body(id_ref, *refs):
    keeps, others, own_w, other_w = refs[0:4], refs[4:8], refs[8:12], refs[12:16]
    mine_ref, theirs_ref, out_ref = refs[16:19]
    c = id_ref[3]
    total = jnp.zeros((HALF, HALF), F32)
    for r in range(4):
        total = total + jnp.dot(keeps[r][...], own_w[r][...], preferred_element_type=F32)
        total = total + jnp.dot(others[r][...], other_w[r][...], preferred_element_type=F32)
    mine = mine_ref[...].astype(F32)
    theirs = theirs_ref[...].astype(F32)
    first = jnp.where(c == 0, mine, theirs)
    second = jnp.where(c == 0, theirs, mine)
    out_ref[...] = (total + jnp.concatenate([first, second], axis=1)).astype(BF)


def feed_body(id_ref, s0, s1, s2, s3, gain_ref, own_ref, other_ref, o0, o1, o2, o3,
              weights, blocks, sems):
    x = id_ref[2]
    copies = []
    for side, ref in enumerate((own_ref, other_ref)):
        for part in range(3):
            copy = pltpu.make_async_copy(
                ref.at[:, pl.ds(64 * part, 64), :], weights.at[side, part], sems.at[side, part]
            )
            copy.start()
            copies.append(copy)
    square = jnp.zeros((HALF, 1), F32)
    for r, s in enumerate((s0, s1, s2, s3)):
        wide = s[...].astype(F32)
        square = square + jnp.sum(wide * wide, axis=1, keepdims=True)
        blocks[lax.rem(x - r + 4, 4)] = s[...]
    scale = lax.rsqrt(square * (1.0 / 2048) + EPSILON)
    normed = jnp.concatenate(
        [
            (blocks[k].astype(F32) * scale * gain_ref[:, 512 * k : 512 * (k + 1)].astype(F32)).astype(BF)
            for k in range(4)
        ],
        axis=1,
    )
    hiddens = []
    for side in range(2):
        copies[3 * side].wait()
        gate = jnp.dot(
            normed, weights[side, 0].reshape(2048, FFD), preferred_element_type=F32
        )
        copies[3 * side + 1].wait()
        up = jnp.dot(
            normed, weights[side, 1].reshape(2048, FFD), preferred_element_type=F32
        )
        hiddens.append((gate * jax.nn.sigmoid(gate) * up).astype(BF))
    copies[2].wait()
    copies[5].wait()
    for r, out in ((1, o1), (3, o3), (2, o2), (0, o0)):
        begin = lax.rem(x + r, 4) * 8
        total = jnp.zeros((HALF, HALF), F32)
        for side in range(2):
            block = weights[side, 2, pl.ds(begin, 8)].reshape(512, FFD)
            total = total + lax.dot_general(
                hiddens[side], block, (((1,), (1,)), ((), ())), preferred_element_type=F32
            )
        out[...] = total.astype(BF)


def mix_body(id_ref, stream_ref, p0, p1, p2, p3, keep_ref, send_ref):
    c = id_ref[3]
    total = p0[...].astype(F32) + p1[...].astype(F32) + p2[...].astype(F32) + p3[...].astype(F32)
    mixed = (stream_ref[...].astype(F32) + 0.5 * total).astype(BF)
    left, right = mixed[:, 0:256], mixed[:, 256:512]
    keep_ref[...] = jnp.where(c == 0, left, right)
    send_ref[...] = jnp.where(c == 0, right, left)


def shift(array, axis, count, by):
    return lax.ppermute(array, axis, [(i, (i + by) % count) for i in range(count)])


def ahead(array, axis, count, by):
    return lax.ppermute(array, axis, [(i, i + by) for i in range(count - by)])


def swap(array):
    return lax.ppermute(array, "c", [(0, 1), (1, 0)])


def around(array):
    return [array] + [shift(array, "x", 4, r) for r in (1, 2, 3)]


def local(
    queries,
    cell_key_rows,
    cell_value_rows,
    output_gate_logits,
    input_gate_logits,
    forget_gate_logits,
    forget_extra_term,
    residual,
    head_norm_gain,
    cell_output_weight,
    feedforward_norm_gain,
    gate_projection_weight,
    up_projection_weight,
    down_projection_weight,
):
    z, y, x, c = (lax.axis_index(n) for n in ("z", "y", "x", "c"))
    place = jnp.stack([z, y, x, c]).astype(jnp.int32)

    shard = jnp.concatenate(
        [gate_projection_weight, up_projection_weight, down_projection_weight.T], axis=0
    )
    own_weights = lax.all_gather(shard, SP)
    other_weights = swap(own_weights)

    message, levels = call(
        summary_body,
        (shape((MSG, DV)), shape((2, 8, 128), F32)),
        (cell_key_rows, cell_value_rows, input_gate_logits, forget_gate_logits, forget_extra_term),
        name="summary",
    )
    near = [shift(message, "y", 4, r) for r in (1, 2, 3)]
    numerator = call(
        inside_body,
        shape((ROWS, DV), F32),
        (queries, cell_key_rows, cell_value_rows, levels),
        flops=2000000000,
        name="inside",
    )
    plane, prefix = call(
        plane_body,
        (shape((MSG, DV)), shape((MSG, DV), F32)),
        (place, message, *near),
        in_specs=[SMEM] + [VMEM] * 4,
        name="plane",
    )
    far = [ahead(plane, "z", 8, r) for r in range(1, 8)]

    halves = residual.reshape(2, HALF, 256)
    residual_mine = lax.dynamic_index_in_dim(halves, c, 0, keepdims=False)
    residual_theirs = swap(lax.dynamic_index_in_dim(halves, 1 - c, 0, keepdims=False))
    own_rows = []
    for r in range(4):
        begin = lax.rem(x + r, 4) * 512
        cut = lax.dynamic_slice_in_dim(cell_output_weight, begin, 512, 1)
        own_rows.append(cut if r == 0 else shift(cut, "x", 4, r))
    other_rows = [swap(rows) for rows in own_rows]

    keep, send = call(
        gated_body,
        (shape((HALF, DV)), shape((HALF, DV))),
        (place, *far, prefix, numerator, queries, levels, output_gate_logits,
         head_norm_gain.reshape(1, DV)),
        in_specs=[SMEM] + [VMEM] * 13,
        name="gated",
    )
    other = swap(send)
    keeps = around(keep)
    others = around(other)
    stream = call(
        stream_body,
        shape((HALF, HALF)),
        (place, *keeps, *others, *own_rows, *other_rows, residual_mine, residual_theirs),
        in_specs=[SMEM] + [VMEM] * 18,
        name="stream",
    )
    streams = around(stream)
    parts = call(
        feed_body,
        tuple(shape((HALF, HALF)) for _ in range(4)),
        (place, *streams, feedforward_norm_gain.reshape(1, 2048), own_weights, other_weights),
        in_specs=[SMEM] + [VMEM] * 5 + [ANY] * 2,
        scratch=(
            pltpu.VMEM((2, 3, 32, 64, FFD), BF),
            pltpu.VMEM((4, HALF, HALF), BF),
            pltpu.SemaphoreType.DMA((2, 3)),
        ),
        flops=9000000000,
        name="feed",
    )
    arrived = [parts[0]] + [shift(parts[r], "x", 4, r) for r in (1, 2, 3)]
    mine, theirs = call(
        mix_body,
        (shape((HALF, 256)), shape((HALF, 256))),
        (place, stream, *arrived),
        in_specs=[SMEM] + [VMEM] * 5,
        name="mix",
    )
    theirs = swap(theirs)
    return jnp.where(
        c == 0, jnp.concatenate([mine, theirs], axis=0), jnp.concatenate([theirs, mine], axis=0)
    )


def solution(mesh):
    torus = Mesh(mesh.devices.reshape(8, 4, 4, 2), ("z", "y", "x", "c"))
    in_specs = (
        P(SP, TP),
        P(SP, TP),
        P(SP, TP),
        P(SP, TP),
        P(TP, SP),
        P(TP, SP),
        P(TP, SP),
        P(SP, TP),
        P(TP),
        P(TP, None),
        P(),
        P(SP, TP),
        P(SP, TP),
        P(TP, SP),
    )
    out_specs = P(SP, TP)
    return jax.shard_map(local, mesh=torus, in_specs=in_specs, out_specs=out_specs, check_vma=False)
```

```python
import functools

import jax
import jax.numpy as jnp
from jax import lax
from jax.experimental import pallas as pl
from jax.experimental.pallas import tpu as pltpu
from jax.sharding import Mesh
from jax.sharding import PartitionSpec as P


SP = ("z", "y")
TP = ("x", "c")
BF = jnp.bfloat16
F32 = jnp.float32
LOWEST = -1e30
EPSILON = 1e-06
ROWS = 1024
HALF = 512
DK = 128
DV = 256
MSG = 144
FFD = 704

VMEM = pl.BlockSpec(memory_space=pltpu.VMEM)
SMEM = pl.BlockSpec(memory_space=pltpu.SMEM)
ANY = pl.BlockSpec(memory_space=pl.ANY)


def call(body, outs, ins, scratch=(), flops=1000000, in_specs=None, vmem=12):
    return pl.pallas_call(
        body,
        out_shape=outs,
        in_specs=in_specs or [VMEM] * len(ins),
        out_specs=jax.tree.map(lambda _: VMEM, outs),
        scratch_shapes=list(scratch),
        cost_estimate=pl.CostEstimate(flops=flops, bytes_accessed=1000000, transcendentals=0),
        compiler_params=pltpu.CompilerParams(vmem_limit_bytes=vmem * 1024 * 1024),
    )(*ins)


def shape(dims, dtype=BF):
    return jax.ShapeDtypeStruct(dims, dtype)


def scan_rows(values, combine, fill):
    lane = lax.broadcasted_iota(jnp.int32, (8, 128), 1)
    row = lax.broadcasted_iota(jnp.int32, (8, 128), 0)
    for step in (1, 2, 4, 8, 16, 32, 64):
        moved = pltpu.roll(values, step, 1)
        values = combine(values, jnp.where(lane >= step, moved, fill))
    last = jnp.broadcast_to(values[:, 127:128], (8, 128))
    before = jnp.where(row >= 1, pltpu.roll(last, 1, 0), fill)
    for step in (1, 2, 4):
        moved = pltpu.roll(before, step, 0)
        before = combine(before, jnp.where(row >= step, moved, fill))
    return combine(values, before)


def eight_rows(ref):
    wide = ref[...].astype(F32)
    return jnp.concatenate([wide[:, 128 * k : 128 * (k + 1)] for k in range(8)], axis=0)


def as_column(values, k):
    return jnp.transpose(jnp.broadcast_to(values[k : k + 1, :], (128, 128)))


def split3(value):
    high = value.astype(BF).astype(F32)
    middle = (value - high).astype(BF).astype(F32)
    return high, middle, value - high - middle


def scalar_tile(top, total, width=256):
    row = lax.broadcasted_iota(jnp.int32, (16, width), 0)
    tile = jnp.zeros((16, width), F32)
    for k, part in enumerate(split3(top) + split3(total)):
        tile = jnp.where(row == k, jnp.broadcast_to(part, (16, width)), tile)
    return tile.astype(BF)


def read_message(ref):
    tile = ref[DK:MSG, :].astype(F32)
    top = tile[0:1] + tile[1:2] + tile[2:3]
    total = tile[3:4] + tile[4:5] + tile[5:6]
    return ref[0:DK, :].astype(F32), top, total


def summary_body(k_ref, v_ref, ig_ref, fg_ref, fe_ref, msg_ref, a_ref):
    gate = eight_rows(ig_ref)
    forget = eight_rows(fg_ref)
    extra = eight_rows(fe_ref)
    small = jnp.exp(-jnp.abs(forget))
    series = small * (1.0 - small * (0.5 - small * (1 / 3 - small * (0.25 - small * 0.2))))
    log_one = jnp.where(small < 0.03, series, jnp.log(1.0 + small))
    log_forget = jnp.minimum(forget, 0.0) - log_one + extra
    running = scan_rows(log_forget, jnp.add, 0.0)
    level = gate - running
    highest = scan_rows(level, jnp.maximum, LOWEST)
    a_ref[0] = level
    a_ref[1] = highest
    final = jnp.broadcast_to(highest[7:8, 127:128], (8, 128))
    weight = jnp.exp(level - final)
    total = jnp.zeros((DK, DV), F32)
    for b in range(8):
        rows = slice(128 * b, 128 * (b + 1))
        scaled = (k_ref[rows, :].astype(F32) * as_column(weight, b)).astype(BF)
        total = total + lax.dot_general(
            scaled, v_ref[rows, :], (((0,), (0,)), ((), ())), preferred_element_type=F32
        )
    msg_ref[0:DK, :] = total.astype(BF)
    all_forget = running[7:8, 127:128]
    msg_ref[DK:MSG, :] = scalar_tile(highest[7:8, 127:128] + all_forget, all_forget)


def inside_body(q_ref, k_ref, v_ref, a_ref, num_ref):
    level = a_ref[0]
    highest = a_ref[1]
    t = lax.broadcasted_iota(jnp.int32, (256, 256), 0)
    s = lax.broadcasted_iota(jnp.int32, (256, 256), 1)
    causal = t >= s
    for i in range(4):
        left = jnp.concatenate([as_column(highest, 2 * i), as_column(highest, 2 * i + 1)], axis=0)
        column = jnp.concatenate([left, left], axis=1)
        query = q_ref[256 * i : 256 * (i + 1), :]
        total = jnp.zeros((256, DV), F32)
        for j in range(i + 1):
            rows = slice(256 * j, 256 * (j + 1))
            line = jnp.concatenate([level[2 * j : 2 * j + 1], level[2 * j + 1 : 2 * j + 2]], axis=1)
            score = lax.dot_general(
                query, k_ref[rows, :], (((1,), (1,)), ((), ())), preferred_element_type=F32
            )
            weight = jnp.exp(line - column)
            if i == j:
                weight = jnp.where(causal, weight, 0.0)
            total = total + jnp.dot(
                (score * weight).astype(BF), v_ref[rows, :], preferred_element_type=F32
            )
        num_ref[256 * i : 256 * (i + 1), :] = total


def plane_body(id_ref, m0, m1, m2, m3, plane_ref, prefix_ref):
    y = id_ref[1]
    parts = [read_message(m) for m in (m0, m1, m2, m3)]
    place = [lax.rem(y - r + 4, 4) for r in range(4)]
    levels, befores = [], []
    total_all = jnp.zeros((1, DV), F32)
    total_before = jnp.zeros((1, DV), F32)
    for r in range(4):
        level = parts[r][1]
        before = parts[r][1]
        for w in range(4):
            if w != r:
                later = place[w] > place[r]
                level = level + jnp.where(later, parts[w][2], 0.0)
                before = before + jnp.where(later & (place[w] < y), parts[w][2], 0.0)
        levels.append(level)
        befores.append(jnp.where(place[r] < y, before, LOWEST))
        total_all = total_all + parts[r][2]
        total_before = total_before + jnp.where(place[r] < y, parts[r][2], 0.0)
    top = functools.reduce(jnp.maximum, levels)
    top_before = functools.reduce(jnp.maximum, befores)
    whole = jnp.zeros((DK, DV), F32)
    early = jnp.zeros((DK, DV), F32)
    for r in range(4):
        whole = whole + jnp.exp(levels[r] - top) * parts[r][0]
        share = jnp.where(place[r] < y, jnp.exp(befores[r] - top_before), 0.0)
        early = early + share * parts[r][0]
    plane_ref[0:DK, :] = whole.astype(BF)
    plane_ref[DK:MSG, :] = scalar_tile(top, total_all)
    prefix_ref[0:DK, :] = early
    prefix_ref[DK : DK + 8, :] = jnp.broadcast_to(top_before, (8, DV))
    prefix_ref[DK + 8 : DK + 16, :] = jnp.broadcast_to(total_before, (8, DV))


def gated_body(
    id_ref, m1, m2, m3, m4, m5, m6, m7, prefix_ref, num_ref, q_ref, a_ref, o_ref, gain_ref, res_ref,
    *outs,
):
    z = id_ref[0]
    x = id_ref[2]
    c = id_ref[3]
    top_before = prefix_ref[DK : DK + 1, :]
    moved = prefix_ref[DK + 8 : DK + 9, :]
    levels = []
    states = []
    for r, m in enumerate((m1, m2, m3, m4, m5, m6, m7)):
        state, top, total = read_message(m)
        levels.append(jnp.where(z > r, top + moved, LOWEST))
        moved = moved + jnp.where(z > r, total, 0.0)
        states.append(state)
    top = functools.reduce(jnp.maximum, levels, top_before)
    carried = jnp.exp(top_before - top) * prefix_ref[0:DK, :]
    for r in range(7):
        share = jnp.where(z > r, jnp.exp(levels[r] - top), 0.0)
        carried = carried + share * states[r]
    high = carried.astype(BF)
    gain = gain_ref[...].astype(F32)
    for r in (2, 1, 3, 0):
        for side, out in ((c, outs[r]), (1 - c, outs[4 + r])):
            group = side * 4 + lax.rem(x + r, 4)
            rows = pl.ds(pl.multiple_of(group * 128, 128), 128)
            line = jnp.broadcast_to(a_ref[1, pl.ds(group, 1), :], (128, 128))
            left = jnp.transpose(line)
            inner = jnp.concatenate([left, left], axis=1)
            row_max = jnp.maximum(inner, top)
            outer = jnp.dot(q_ref[rows, :], high, preferred_element_type=F32)
            memory = jnp.exp(inner - row_max) * num_ref[rows, :] + jnp.exp(top - row_max) * outer
            memory = memory * (DK**-0.5)
            mean = jnp.sum(memory * memory, axis=1, keepdims=True) * (1.0 / DV)
            normal = memory * lax.rsqrt(mean + EPSILON)
            opened = jax.nn.sigmoid(o_ref[rows, :].astype(F32))
            out[:, 0:256] = (normal * gain * opened).astype(BF)
            out[:, 256:512] = res_ref[rows, :]


def stream_body(id_ref, *refs):
    keeps, others, own_w, other_w = refs[0:4], refs[4:8], refs[8:12], refs[12:16]
    out_ref = refs[16]
    scratch = refs[17]
    x = id_ref[2]
    c = id_ref[3]
    for r in range(4):
        chip = lax.rem(x - r + 4, 4)
        scratch[chip * 2 + c] = keeps[r][:, 256:512]
        scratch[chip * 2 + 1 - c] = others[r][:, 256:512]
    for n in range(4):
        cols = slice(512 * n, 512 * (n + 1))
        total = jnp.concatenate(
            [scratch[2 * n].astype(F32), scratch[2 * n + 1].astype(F32)], axis=1
        )
        for r in range(4):
            total = total + jnp.dot(
                keeps[r][:, 0:256], own_w[r][:, cols], preferred_element_type=F32
            )
            total = total + jnp.dot(
                others[r][:, 0:256], other_w[r][:, cols], preferred_element_type=F32
            )
        out_ref[:, cols] = total.astype(BF)


def feed_body(id_ref, s0, s1, s2, s3, gain_ref, w_ref, o0, o1, o2, o3, weights, blocks, sems):
    x = id_ref[2]
    copies = []
    for side in range(2):
        made = []
        for part in range(3):
            copy = pltpu.make_async_copy(
                w_ref.at[:, side, pl.ds(64 * part, 64), :],
                weights.at[side, :, pl.ds(64 * part, 64), :],
                sems.at[side, part],
            )
            copy.start()
            made.append(copy)
        copies.append(made)
    for r, s in enumerate((s0, s1, s2, s3)):
        blocks[lax.rem(x - r + 4, 4)] = s[...]
    wide = blocks[...].reshape(HALF, 2048).astype(F32)
    square = jnp.sum(wide * wide, axis=1, keepdims=True)
    scale = lax.rsqrt(square * (1.0 / 2048) + EPSILON)
    normed = (wide * scale * gain_ref[...].astype(F32)).astype(BF)
    hiddens = []
    for side in range(2):
        copies[side][0].wait()
        gate = jnp.dot(
            normed, weights[side, :, 0:64, :].reshape(2048, FFD), preferred_element_type=F32
        )
        copies[side][1].wait()
        up = jnp.dot(
            normed, weights[side, :, 64:128, :].reshape(2048, FFD), preferred_element_type=F32
        )
        hiddens.append((gate * jax.nn.sigmoid(gate) * up).astype(BF))
    copies[0][2].wait()
    copies[1][2].wait()
    for r, out in ((2, o2), (1, o1), (3, o3), (0, o0)):
        begin = lax.rem(x + r, 4) * 8
        total = jnp.zeros((HALF, HALF), F32)
        for side in range(2):
            block = weights[side, pl.ds(begin, 8), 128:192, :].reshape(512, FFD)
            total = total + lax.dot_general(
                hiddens[side], block, (((1,), (1,)), ((), ())), preferred_element_type=F32
            )
        if r == 0:
            cols = pl.ds(pl.multiple_of(x * 512, 512), 512)
            out[...] = 0.5 * total + blocks[:, :, cols].reshape(HALF, HALF).astype(F32)
        else:
            out[...] = total.astype(BF)


def mix_body(id_ref, p0, p1, p2, p3, whole_ref, send_ref):
    c = id_ref[3]
    total = p1[...].astype(F32) + p2[...].astype(F32) + p3[...].astype(F32)
    mixed = (p0[...] + 0.5 * total).astype(BF)
    left, right = mixed[:, 0:256], mixed[:, 256:512]
    mine = jnp.where(c == 0, left, right)
    whole_ref[0:HALF, :] = mine
    whole_ref[HALF:ROWS, :] = mine
    send_ref[...] = jnp.where(c == 0, right, left)


def shift(array, axis, count, by):
    return lax.ppermute(array, axis, [(i, (i + by) % count) for i in range(count)])


def ahead(array, axis, count, by):
    return lax.ppermute(array, axis, [(i, i + by) for i in range(count - by)])


def swap(array):
    return lax.ppermute(array, "c", [(0, 1), (1, 0)])


def cross(array, by):
    pairs = []
    for i in range(4):
        for j in range(2):
            pairs.append((2 * i + j, 2 * ((i + by) % 4) + 1 - j))
    return lax.ppermute(array, TP, pairs)


def spread(array, axis):
    return [array] + [shift(array, axis, 4, r) for r in (1, 2, 3)]


def layer(
    queries,
    cell_key_rows,
    cell_value_rows,
    output_gate_logits,
    input_gate_logits,
    forget_gate_logits,
    forget_extra_term,
    residual,
    head_norm_gain,
    cell_output_weight,
    feedforward_norm_gain,
    gate_projection_weight,
    up_projection_weight,
    down_projection_weight,
):
    z, y, x, c = (lax.axis_index(n) for n in ("z", "y", "x", "c"))
    place = jnp.stack([z, y, x, c]).astype(jnp.int32)

    own_out = spread(cell_output_weight, "x")
    other_out = [swap(rows) for rows in own_out]

    message, levels = call(
        summary_body,
        (shape((MSG, DV)), shape((2, 8, 128), F32)),
        (cell_key_rows, cell_value_rows, input_gate_logits, forget_gate_logits, forget_extra_term),
    )
    near = spread(message, "y")[1:]

    shard = jnp.concatenate(
        [gate_projection_weight, up_projection_weight, down_projection_weight.T], axis=0
    )
    weights = lax.all_gather(shard, ("z", "y", "c")).reshape(32, 2, 192, FFD)

    numerator = call(
        inside_body,
        shape((ROWS, DV), F32),
        (queries, cell_key_rows, cell_value_rows, levels),
        flops=2000000000,
    )
    plane, prefix = call(
        plane_body,
        (shape((MSG, DV)), shape((MSG, DV), F32)),
        (place, message, *near),
        in_specs=[SMEM] + [VMEM] * 4,
    )
    far = [ahead(plane, "z", 8, r) for r in range(1, 8)]
    gated = call(
        gated_body,
        tuple(shape((128, 512)) for _ in range(8)),
        (place, *far, prefix, numerator, queries, levels, output_gate_logits,
         head_norm_gain.reshape(1, DV), residual),
        in_specs=[SMEM] + [VMEM] * 14,
    )
    keeps = [gated[0]] + [shift(gated[r], "x", 4, r) for r in (1, 2, 3)]
    others = [cross(gated[4 + r], r) for r in range(4)]
    stream = call(
        stream_body,
        shape((128, 2048)),
        (place, *keeps, *others, *own_out, *other_out),
        in_specs=[SMEM] + [VMEM] * 16,
        scratch=(pltpu.VMEM((8, 128, 256), BF),),
        vmem=20,
    )
    streams = spread(stream, "x")
    parts = call(
        feed_body,
        (shape((HALF, HALF), F32),) + tuple(shape((HALF, HALF)) for _ in range(3)),
        (place, *streams, feedforward_norm_gain.reshape(1, 2048), weights),
        in_specs=[SMEM] + [VMEM] * 5 + [ANY],
        scratch=(
            pltpu.VMEM((2, 32, 192, FFD), BF),
            pltpu.VMEM((4, 128, 2048), BF),
            pltpu.SemaphoreType.DMA((2, 3)),
        ),
        flops=9000000000,
        vmem=58,
    )
    arrived = [parts[0]] + [shift(parts[r], "x", 4, r) for r in (1, 2, 3)]
    whole, theirs = call(
        mix_body,
        (shape((ROWS, 256)), shape((HALF, 256))),
        (place, *arrived),
        in_specs=[SMEM] + [VMEM] * 4,
    )
    return lax.dynamic_update_slice(whole, swap(theirs), ((1 - c) * HALF, jnp.int32(0)))


def solution(mesh):
    torus = Mesh(mesh.devices.reshape(8, 4, 4, 2), ("z", "y", "x", "c"))
    in_specs = (
        P(SP, TP),
        P(SP, TP),
        P(SP, TP),
        P(SP, TP),
        P(TP, SP),
        P(TP, SP),
        P(TP, SP),
        P(SP, TP),
        P(TP),
        P(TP, None),
        P(),
        P(SP, TP),
        P(SP, TP),
        P(TP, SP),
    )
    out_specs = P(SP, TP)
    return jax.shard_map(layer, mesh=torus, in_specs=in_specs, out_specs=out_specs, check_vma=False)
```

```python
import functools

import jax
import jax.numpy as jnp
from jax import lax
from jax.experimental import pallas as pl
from jax.experimental.pallas import tpu as pltpu
from jax.sharding import Mesh
from jax.sharding import PartitionSpec as P


SP = ("z", "y")
TP = ("x", "c")
BF = jnp.bfloat16
F32 = jnp.float32
LOWEST = -1e30
EPSILON = 1e-06
ROWS = 1024
HALF = 512
DK = 128
DV = 256
MSG = 144
FFD = 704

VMEM = pl.BlockSpec(memory_space=pltpu.VMEM)
SMEM = pl.BlockSpec(memory_space=pltpu.SMEM)
ANY = pl.BlockSpec(memory_space=pl.ANY)


def call(body, outs, ins, scratch=(), flops=1000000, in_specs=None, vmem=12):
    return pl.pallas_call(
        body,
        out_shape=outs,
        in_specs=in_specs or [VMEM] * len(ins),
        out_specs=jax.tree.map(lambda _: VMEM, outs),
        scratch_shapes=list(scratch),
        cost_estimate=pl.CostEstimate(flops=flops, bytes_accessed=1000000, transcendentals=0),
        compiler_params=pltpu.CompilerParams(vmem_limit_bytes=vmem * 1024 * 1024),
    )(*ins)


def shape(dims, dtype=BF):
    return jax.ShapeDtypeStruct(dims, dtype)


def scan_rows(values, combine, fill):
    lane = lax.broadcasted_iota(jnp.int32, (8, 128), 1)
    row = lax.broadcasted_iota(jnp.int32, (8, 128), 0)
    for step in (1, 2, 4, 8, 16, 32, 64):
        moved = pltpu.roll(values, step, 1)
        values = combine(values, jnp.where(lane >= step, moved, fill))
    last = jnp.broadcast_to(values[:, 127:128], (8, 128))
    before = jnp.where(row >= 1, pltpu.roll(last, 1, 0), fill)
    for step in (1, 2, 4):
        moved = pltpu.roll(before, step, 0)
        before = combine(before, jnp.where(row >= step, moved, fill))
    return combine(values, before)


def eight_rows(ref):
    wide = ref[...].astype(F32)
    return jnp.concatenate([wide[:, 128 * k : 128 * (k + 1)] for k in range(8)], axis=0)


def as_column(values, k):
    return jnp.transpose(jnp.broadcast_to(values[k : k + 1, :], (128, 128)))


def split3(value):
    high = value.astype(BF).astype(F32)
    middle = (value - high).astype(BF).astype(F32)
    return high, middle, value - high - middle


def scalar_tile(top, total, width=256):
    row = lax.broadcasted_iota(jnp.int32, (16, width), 0)
    tile = jnp.zeros((16, width), F32)
    for k, part in enumerate(split3(top) + split3(total)):
        tile = jnp.where(row == k, jnp.broadcast_to(part, (16, width)), tile)
    return tile.astype(BF)


def read_message(ref):
    tile = ref[DK:MSG, :].astype(F32)
    top = tile[0:1] + tile[1:2] + tile[2:3]
    total = tile[3:4] + tile[4:5] + tile[5:6]
    return ref[0:DK, :].astype(F32), top, total


def summary_body(k_ref, v_ref, ig_ref, fg_ref, fe_ref, msg_ref, a_ref):
    gate = eight_rows(ig_ref)
    forget = eight_rows(fg_ref)
    extra = eight_rows(fe_ref)
    small = jnp.exp(-jnp.abs(forget))
    series = small * (1.0 - small * (0.5 - small * (1 / 3 - small * (0.25 - small * 0.2))))
    log_one = jnp.where(small < 0.03, series, jnp.log(1.0 + small))
    log_forget = jnp.minimum(forget, 0.0) - log_one + extra
    running = scan_rows(log_forget, jnp.add, 0.0)
    level = gate - running
    highest = scan_rows(level, jnp.maximum, LOWEST)
    a_ref[0] = level
    a_ref[1] = highest
    final = jnp.broadcast_to(highest[7:8, 127:128], (8, 128))
    weight = jnp.exp(level - final)
    total = jnp.zeros((DK, DV), F32)
    for b in range(8):
        rows = slice(128 * b, 128 * (b + 1))
        scaled = (k_ref[rows, :].astype(F32) * as_column(weight, b)).astype(BF)
        total = total + lax.dot_general(
            scaled, v_ref[rows, :], (((0,), (0,)), ((), ())), preferred_element_type=F32
        )
    msg_ref[0:DK, :] = total.astype(BF)
    all_forget = running[7:8, 127:128]
    msg_ref[DK:MSG, :] = scalar_tile(highest[7:8, 127:128] + all_forget, all_forget)


def inside_body(q_ref, k_ref, v_ref, a_ref, num_ref):
    level = a_ref[0]
    highest = a_ref[1]
    t = lax.broadcasted_iota(jnp.int32, (256, 256), 0)
    s = lax.broadcasted_iota(jnp.int32, (256, 256), 1)
    causal = t >= s
    for i in range(4):
        left = jnp.concatenate([as_column(highest, 2 * i), as_column(highest, 2 * i + 1)], axis=0)
        column = jnp.concatenate([left, left], axis=1)
        query = q_ref[256 * i : 256 * (i + 1), :]
        total = jnp.zeros((256, DV), F32)
        for j in range(i + 1):
            rows = slice(256 * j, 256 * (j + 1))
            line = jnp.concatenate([level[2 * j : 2 * j + 1], level[2 * j + 1 : 2 * j + 2]], axis=1)
            score = lax.dot_general(
                query, k_ref[rows, :], (((1,), (1,)), ((), ())), preferred_element_type=F32
            )
            weight = jnp.exp(line - column)
            if i == j:
                weight = jnp.where(causal, weight, 0.0)
            total = total + jnp.dot(
                (score * weight).astype(BF), v_ref[rows, :], preferred_element_type=F32
            )
        num_ref[256 * i : 256 * (i + 1), :] = total


def plane_body(id_ref, m0, m1, m2, m3, plane_ref, prefix_ref):
    y = id_ref[1]
    parts = [read_message(m) for m in (m0, m1, m2, m3)]
    place = [lax.rem(y - r + 4, 4) for r in range(4)]
    levels, befores = [], []
    total_all = jnp.zeros((1, DV), F32)
    total_before = jnp.zeros((1, DV), F32)
    for r in range(4):
        level = parts[r][1]
        before = parts[r][1]
        for w in range(4):
            if w != r:
                later = place[w] > place[r]
                level = level + jnp.where(later, parts[w][2], 0.0)
                before = before + jnp.where(later & (place[w] < y), parts[w][2], 0.0)
        levels.append(level)
        befores.append(jnp.where(place[r] < y, before, LOWEST))
        total_all = total_all + parts[r][2]
        total_before = total_before + jnp.where(place[r] < y, parts[r][2], 0.0)
    top = functools.reduce(jnp.maximum, levels)
    top_before = functools.reduce(jnp.maximum, befores)
    whole = jnp.zeros((DK, DV), F32)
    early = jnp.zeros((DK, DV), F32)
    for r in range(4):
        whole = whole + jnp.exp(levels[r] - top) * parts[r][0]
        share = jnp.where(place[r] < y, jnp.exp(befores[r] - top_before), 0.0)
        early = early + share * parts[r][0]
    plane_ref[0:DK, :] = whole.astype(BF)
    plane_ref[DK:MSG, :] = scalar_tile(top, total_all)
    prefix_ref[0:DK, :] = early
    prefix_ref[DK : DK + 8, :] = jnp.broadcast_to(top_before, (8, DV))
    prefix_ref[DK + 8 : DK + 16, :] = jnp.broadcast_to(total_before, (8, DV))


def join_body(id_ref, near_ref, far_ref, out_ref):
    z, y = id_ref[0], id_ref[1]
    state_near, top_near, total_near = read_message(near_ref)
    state_far, top_far, total_far = read_message(far_ref)
    has_near = z >= 2 * y + 1
    has_far = (z >= 2 * y + 2) & (y < 3)
    top_near = jnp.where(has_near, top_near, LOWEST)
    total_near = jnp.where(has_near, total_near, 0.0)
    moved = jnp.where(has_far, top_far + total_near, LOWEST)
    total_far = jnp.where(has_far, total_far, 0.0)
    top = jnp.maximum(top_near, moved)
    share_near = jnp.where(has_near, jnp.exp(top_near - top), 0.0)
    share_far = jnp.where(has_far, jnp.exp(moved - top), 0.0)
    out_ref[0:DK, :] = (share_near * state_near + share_far * state_far).astype(BF)
    out_ref[DK:MSG, :] = scalar_tile(top, total_near + total_far)


def gated_body(
    id_ref, m0, m1, m2, m3, prefix_ref, num_ref, q_ref, a_ref, o_ref, gain_ref, res_ref, *outs
):
    y = id_ref[1]
    x = id_ref[2]
    c = id_ref[3]
    top_before = prefix_ref[DK : DK + 1, :]
    parts = [read_message(m) for m in (m0, m1, m2, m3)]
    place = [lax.rem(y - r + 4, 4) for r in range(4)]
    levels = []
    for r in range(4):
        level = parts[r][1] + prefix_ref[DK + 8 : DK + 9, :]
        for w in range(4):
            if w != r:
                level = level + jnp.where(place[w] < place[r], parts[w][2], 0.0)
        levels.append(level)
    top = functools.reduce(jnp.maximum, levels, top_before)
    carried = jnp.exp(top_before - top) * prefix_ref[0:DK, :]
    for r in range(4):
        carried = carried + jnp.exp(levels[r] - top) * parts[r][0]
    high = carried.astype(BF)
    gain = gain_ref[...].astype(F32)
    for r in (2, 1, 3, 0):
        for side, out in ((c, outs[r]), (1 - c, outs[4 + r])):
            group = side * 4 + lax.rem(x + r, 4)
            rows = pl.ds(pl.multiple_of(group * 128, 128), 128)
            line = jnp.broadcast_to(a_ref[1, pl.ds(group, 1), :], (128, 128))
            left = jnp.transpose(line)
            inner = jnp.concatenate([left, left], axis=1)
            row_max = jnp.maximum(inner, top)
            outer = jnp.dot(q_ref[rows, :], high, preferred_element_type=F32)
            memory = jnp.exp(inner - row_max) * num_ref[rows, :] + jnp.exp(top - row_max) * outer
            memory = memory * (DK**-0.5)
            mean = jnp.sum(memory * memory, axis=1, keepdims=True) * (1.0 / DV)
            normal = memory * lax.rsqrt(mean + EPSILON)
            opened = jax.nn.sigmoid(o_ref[rows, :].astype(F32))
            out[:, 0:256] = (normal * gain * opened).astype(BF)
            out[:, 256:512] = res_ref[rows, :]


def stream_body(id_ref, *refs):
    keeps, others, own_w, other_w = refs[0:4], refs[4:8], refs[8:12], refs[12:16]
    out_ref = refs[16]
    scratch = refs[17]
    x = id_ref[2]
    c = id_ref[3]
    for r in range(4):
        chip = lax.rem(x - r + 4, 4)
        scratch[chip * 2 + c] = keeps[r][:, 256:512]
        scratch[chip * 2 + 1 - c] = others[r][:, 256:512]
    for n in range(4):
        cols = slice(512 * n, 512 * (n + 1))
        total = jnp.concatenate(
            [scratch[2 * n].astype(F32), scratch[2 * n + 1].astype(F32)], axis=1
        )
        for r in range(4):
            total = total + jnp.dot(
                keeps[r][:, 0:256], own_w[r][:, cols], preferred_element_type=F32
            )
            total = total + jnp.dot(
                others[r][:, 0:256], other_w[r][:, cols], preferred_element_type=F32
            )
        out_ref[:, cols] = total.astype(BF)


def norm_body(id_ref, s0, s1, s2, s3, gain_ref, out_ref, own_ref, blocks):
    x = id_ref[2]
    for r, s in enumerate((s0, s1, s2, s3)):
        blocks[lax.rem(x - r + 4, 4)] = s[...]
    gain = gain_ref[...].astype(F32)
    cols = pl.ds(pl.multiple_of(x * 512, 512), 512)
    for k in range(4):
        rows = slice(128 * k, 128 * (k + 1))
        wide = blocks[k].astype(F32)
        square = jnp.sum(wide * wide, axis=1, keepdims=True)
        scale = lax.rsqrt(square * (1.0 / 2048) + EPSILON)
        out_ref[rows, :] = (wide * scale * gain).astype(BF)
        own_ref[rows, :] = blocks[k, :, cols]


def feed_body(id_ref, n_ref, w_ref, hidden_ref, o2, weights, block, sems, other_sems):
    x = id_ref[2]
    begin = lax.rem(x + 2, 4) * 8
    copies = []
    for side in range(2):
        made = []
        for part in range(2):
            copy = pltpu.make_async_copy(
                w_ref.at[:, side, pl.ds(64 * part, 64), :],
                weights.at[side, part],
                sems.at[side, part],
            )
            copy.start()
            made.append(copy)
        copies.append(made)
    downs = []
    for side in range(2):
        copy = pltpu.make_async_copy(
            w_ref.at[pl.ds(begin, 8), side, pl.ds(128, 64), :], block.at[side], other_sems.at[side]
        )
        copy.start()
        downs.append(copy)
    for side in range(2):
        copies[side][0].wait()
        gate = jnp.dot(
            n_ref[...], weights[side, 0].reshape(2048, FFD), preferred_element_type=F32
        )
        copies[side][1].wait()
        up = jnp.dot(n_ref[...], weights[side, 1].reshape(2048, FFD), preferred_element_type=F32)
        hidden_ref[side] = (gate * jax.nn.sigmoid(gate) * up).astype(BF)
    total = jnp.zeros((HALF, HALF), F32)
    for side in range(2):
        downs[side].wait()
        total = total + lax.dot_general(
            hidden_ref[side], block[side].reshape(512, FFD), (((1,), (1,)), ((), ())),
            preferred_element_type=F32,
        )
    o2[...] = total.astype(BF)


def down_body(shifts, id_ref, hidden_ref, w_ref, *refs):
    outs = refs[: len(shifts)]
    block, sems = refs[len(shifts) :]
    x = id_ref[2]
    copies = []
    for n, r in enumerate(shifts):
        begin = lax.rem(x + r, 4) * 8
        for side in range(2):
            copy = pltpu.make_async_copy(
                w_ref.at[pl.ds(begin, 8), side, pl.ds(128, 64), :],
                block.at[n, side],
                sems.at[n, side],
            )
            copy.start()
            copies.append(copy)
    for n in range(len(shifts)):
        total = jnp.zeros((HALF, HALF), F32)
        for side in range(2):
            copies[2 * n + side].wait()
            total = total + lax.dot_general(
                hidden_ref[side], block[n, side].reshape(512, FFD), (((1,), (1,)), ((), ())),
                preferred_element_type=F32,
            )
        outs[n][...] = total.astype(BF)


def down_call(shifts, place, hidden, weights):
    return call(
        functools.partial(down_body, shifts),
        tuple(shape((HALF, HALF)) for _ in shifts),
        (place, hidden, weights),
        in_specs=[SMEM, VMEM, ANY],
        scratch=(
            pltpu.VMEM((len(shifts), 2, 8, 64, FFD), BF),
            pltpu.SemaphoreType.DMA((len(shifts), 2)),
        ),
        flops=1100000000 * len(shifts),
        vmem=60,
    )


def mix_body(id_ref, stream_ref, p0, p1, p2, p3, whole_ref, send_ref):
    c = id_ref[3]
    total = p0[...].astype(F32) + p1[...].astype(F32) + p2[...].astype(F32) + p3[...].astype(F32)
    mixed = (stream_ref[...].astype(F32) + 0.5 * total).astype(BF)
    left, right = mixed[:, 0:256], mixed[:, 256:512]
    mine = jnp.where(c == 0, left, right)
    whole_ref[0:HALF, :] = mine
    whole_ref[HALF:ROWS, :] = mine
    send_ref[...] = jnp.where(c == 0, right, left)


def shift(array, axis, count, by):
    return lax.ppermute(array, axis, [(i, (i + by) % count) for i in range(count)])


def column(array, steps):
    pairs = []
    for y in range(4):
        for z in range(8 - steps[y]):
            pairs.append((4 * z + y, 4 * (z + steps[y]) + y))
    return lax.ppermute(array, SP, pairs)


def swap(array):
    return lax.ppermute(array, "c", [(0, 1), (1, 0)])


def cross(array, by):
    pairs = []
    for i in range(4):
        for j in range(2):
            pairs.append((2 * i + j, 2 * ((i + by) % 4) + 1 - j))
    return lax.ppermute(array, TP, pairs)


def spread(array, axis):
    return [array] + [shift(array, axis, 4, r) for r in (1, 2, 3)]


def layer(
    queries,
    cell_key_rows,
    cell_value_rows,
    output_gate_logits,
    input_gate_logits,
    forget_gate_logits,
    forget_extra_term,
    residual,
    head_norm_gain,
    cell_output_weight,
    feedforward_norm_gain,
    gate_projection_weight,
    up_projection_weight,
    down_projection_weight,
):
    z, y, x, c = (lax.axis_index(n) for n in ("z", "y", "x", "c"))
    place = jnp.stack([z, y, x, c]).astype(jnp.int32)

    own_out = spread(cell_output_weight, "x")
    other_out = [swap(rows) for rows in own_out]

    message, levels = call(
        summary_body,
        (shape((MSG, DV)), shape((2, 8, 128), F32)),
        (cell_key_rows, cell_value_rows, input_gate_logits, forget_gate_logits, forget_extra_term),
        vmem=60,
    )
    near = spread(message, "y")[1:]

    shard = jnp.concatenate(
        [gate_projection_weight, up_projection_weight, down_projection_weight.T], axis=0
    )
    weights = lax.all_gather(shard, ("z", "y", "c")).reshape(32, 2, 192, FFD)

    numerator = call(
        inside_body,
        shape((ROWS, DV), F32),
        (queries, cell_key_rows, cell_value_rows, levels),
        flops=2000000000,
        vmem=60,
    )
    plane, prefix = call(
        plane_body,
        (shape((MSG, DV)), shape((MSG, DV), F32)),
        (place, message, *near),
        in_specs=[SMEM] + [VMEM] * 4,
    )
    joined = call(
        join_body,
        shape((MSG, DV)),
        (place, column(plane, (1, 3, 5, 7)), column(plane, (2, 4, 6, 8))),
        in_specs=[SMEM] + [VMEM] * 2,
    )
    gated = call(
        gated_body,
        tuple(shape((128, 512)) for _ in range(8)),
        (place, *spread(joined, "y"), prefix, numerator, queries, levels,
         output_gate_logits, head_norm_gain.reshape(1, DV), residual),
        in_specs=[SMEM] + [VMEM] * 11,
        vmem=60,
    )
    keeps = [gated[0]] + [shift(gated[r], "x", 4, r) for r in (1, 2, 3)]
    others = [cross(gated[4 + r], r) for r in range(4)]
    stream = call(
        stream_body,
        shape((128, 2048)),
        (place, *keeps, *others, *own_out, *other_out),
        in_specs=[SMEM] + [VMEM] * 16,
        scratch=(pltpu.VMEM((8, 128, 256), BF),),
        vmem=20,
    )
    streams = spread(stream, "x")
    normed, own_stream = call(
        norm_body,
        (shape((HALF, 2048)), shape((HALF, HALF))),
        (place, *streams, feedforward_norm_gain.reshape(1, 2048)),
        in_specs=[SMEM] + [VMEM] * 5,
        scratch=(pltpu.VMEM((4, 128, 2048), BF),),
    )
    hidden, part2 = call(
        feed_body,
        (shape((2, HALF, FFD)), shape((HALF, HALF))),
        (place, normed, weights),
        in_specs=[SMEM, VMEM, ANY],
        scratch=(
            pltpu.VMEM((2, 2, 32, 64, FFD), BF),
            pltpu.VMEM((2, 8, 64, FFD), BF),
            pltpu.SemaphoreType.DMA((2, 2)),
            pltpu.SemaphoreType.DMA((2,)),
        ),
        flops=7000000000,
        vmem=60,
    )
    part1, part3 = down_call((1, 3), place, hidden, weights)
    (part0,) = down_call((0,), place, hidden, weights)
    arrived = [part0] + [shift(part, "x", 4, r) for r, part in ((1, part1), (2, part2), (3, part3))]
    whole, theirs = call(
        mix_body,
        (shape((ROWS, 256)), shape((HALF, 256))),
        (place, own_stream, *arrived),
        in_specs=[SMEM] + [VMEM] * 5,
        vmem=60,
    )
    return lax.dynamic_update_slice(whole, swap(theirs), ((1 - c) * HALF, jnp.int32(0)))


def solution(mesh):
    torus = Mesh(mesh.devices.reshape(8, 4, 4, 2), ("z", "y", "x", "c"))
    in_specs = (
        P(SP, TP),
        P(SP, TP),
        P(SP, TP),
        P(SP, TP),
        P(TP, SP),
        P(TP, SP),
        P(TP, SP),
        P(SP, TP),
        P(TP),
        P(TP, None),
        P(),
        P(SP, TP),
        P(SP, TP),
        P(TP, SP),
    )
    out_specs = P(SP, TP)
    return jax.shard_map(layer, mesh=torus, in_specs=in_specs, out_specs=out_specs, check_vma=False)
```

```python
import functools

import jax
import jax.numpy as jnp
from jax import lax
from jax.experimental import pallas as pl
from jax.experimental.pallas import tpu as pltpu
from jax.sharding import Mesh
from jax.sharding import PartitionSpec as P


SP = ("z", "y")
TP = ("x", "c")
BF = jnp.bfloat16
F32 = jnp.float32
LOWEST = -1e30
EPSILON = 1e-06
ROWS = 1024
HALF = 512
PART = 256
DK = 128
DV = 256
MSG = 144
FFD = 704

VMEM = pl.BlockSpec(memory_space=pltpu.VMEM)
SMEM = pl.BlockSpec(memory_space=pltpu.SMEM)
ANY = pl.BlockSpec(memory_space=pltpu.HBM)


def call(body, outs, ins, scratch=(), flops=1000000, in_specs=None, vmem=12):
    return pl.pallas_call(
        body,
        out_shape=outs,
        in_specs=in_specs or [VMEM] * len(ins),
        out_specs=jax.tree.map(lambda _: VMEM, outs),
        scratch_shapes=list(scratch),
        cost_estimate=pl.CostEstimate(flops=flops, bytes_accessed=1000000, transcendentals=0),
        compiler_params=pltpu.CompilerParams(vmem_limit_bytes=vmem * 1024 * 1024),
    )(*ins)


def shape(dims, dtype=BF):
    return jax.ShapeDtypeStruct(dims, dtype)


def scan_rows(values, combine, fill):
    lane = lax.broadcasted_iota(jnp.int32, (8, 128), 1)
    row = lax.broadcasted_iota(jnp.int32, (8, 128), 0)
    for step in (1, 2, 4, 8, 16, 32, 64):
        moved = pltpu.roll(values, step, 1)
        values = combine(values, jnp.where(lane >= step, moved, fill))
    last = jnp.broadcast_to(values[:, 127:128], (8, 128))
    before = jnp.where(row >= 1, pltpu.roll(last, 1, 0), fill)
    for step in (1, 2, 4):
        moved = pltpu.roll(before, step, 0)
        before = combine(before, jnp.where(row >= step, moved, fill))
    return combine(values, before)


def eight_rows(ref):
    wide = ref[...].astype(F32)
    return jnp.concatenate([wide[:, 128 * k : 128 * (k + 1)] for k in range(8)], axis=0)


def as_column(values, k):
    return jnp.transpose(jnp.broadcast_to(values[k : k + 1, :], (128, 128)))


def split3(value):
    high = value.astype(BF).astype(F32)
    middle = (value - high).astype(BF).astype(F32)
    return high, middle, value - high - middle


def scalar_tile(top, total, width=256):
    row = lax.broadcasted_iota(jnp.int32, (16, width), 0)
    tile = jnp.zeros((16, width), F32)
    for k, part in enumerate(split3(top) + split3(total)):
        tile = jnp.where(row == k, jnp.broadcast_to(part, (16, width)), tile)
    return tile.astype(BF)


def read_message(ref):
    tile = ref[DK:MSG, :].astype(F32)
    top = tile[0:1] + tile[1:2] + tile[2:3]
    total = tile[3:4] + tile[4:5] + tile[5:6]
    return ref[0:DK, :].astype(F32), top, total


def summary_body(k_ref, v_ref, ig_ref, fg_ref, fe_ref, msg_ref, a_ref):
    gate = eight_rows(ig_ref)
    forget = eight_rows(fg_ref)
    extra = eight_rows(fe_ref)
    small = jnp.exp(-jnp.abs(forget))
    series = small * (1.0 - small * (0.5 - small * (1 / 3 - small * (0.25 - small * 0.2))))
    log_one = jnp.where(small < 0.03, series, jnp.log(1.0 + small))
    log_forget = jnp.minimum(forget, 0.0) - log_one + extra
    running = scan_rows(log_forget, jnp.add, 0.0)
    level = gate - running
    highest = scan_rows(level, jnp.maximum, LOWEST)
    a_ref[0] = level
    a_ref[1] = highest
    final = jnp.broadcast_to(highest[7:8, 127:128], (8, 128))
    weight = jnp.exp(level - final)
    total = jnp.zeros((DK, DV), F32)
    for b in range(8):
        rows = slice(128 * b, 128 * (b + 1))
        scaled = (k_ref[rows, :].astype(F32) * as_column(weight, b)).astype(BF)
        total = total + lax.dot_general(
            scaled, v_ref[rows, :], (((0,), (0,)), ((), ())), preferred_element_type=F32
        )
    msg_ref[0:DK, :] = total.astype(BF)
    all_forget = running[7:8, 127:128]
    msg_ref[DK:MSG, :] = scalar_tile(highest[7:8, 127:128] + all_forget, all_forget)


def inside_body(q_ref, k_ref, v_ref, a_ref, num_ref):
    level = a_ref[0]
    highest = a_ref[1]
    t = lax.broadcasted_iota(jnp.int32, (256, 256), 0)
    s = lax.broadcasted_iota(jnp.int32, (256, 256), 1)
    causal = t >= s
    for i in range(4):
        left = jnp.concatenate([as_column(highest, 2 * i), as_column(highest, 2 * i + 1)], axis=0)
        column = jnp.concatenate([left, left], axis=1)
        query = q_ref[256 * i : 256 * (i + 1), :]
        total = jnp.zeros((256, DV), F32)
        for j in range(i + 1):
            rows = slice(256 * j, 256 * (j + 1))
            line = jnp.concatenate([level[2 * j : 2 * j + 1], level[2 * j + 1 : 2 * j + 2]], axis=1)
            score = lax.dot_general(
                query, k_ref[rows, :], (((1,), (1,)), ((), ())), preferred_element_type=F32
            )
            weight = jnp.exp(line - column)
            if i == j:
                weight = jnp.where(causal, weight, 0.0)
            total = total + jnp.dot(
                (score * weight).astype(BF), v_ref[rows, :], preferred_element_type=F32
            )
        num_ref[256 * i : 256 * (i + 1), :] = total


def plane_body(id_ref, m0, m1, m2, m3, plane_ref, prefix_ref):
    y = id_ref[1]
    parts = [read_message(m) for m in (m0, m1, m2, m3)]
    place = [lax.rem(y - r + 4, 4) for r in range(4)]
    levels, befores = [], []
    total_all = jnp.zeros((1, DV), F32)
    total_before = jnp.zeros((1, DV), F32)
    for r in range(4):
        level = parts[r][1]
        before = parts[r][1]
        for w in range(4):
            if w != r:
                later = place[w] > place[r]
                level = level + jnp.where(later, parts[w][2], 0.0)
                before = before + jnp.where(later & (place[w] < y), parts[w][2], 0.0)
        levels.append(level)
        befores.append(jnp.where(place[r] < y, before, LOWEST))
        total_all = total_all + parts[r][2]
        total_before = total_before + jnp.where(place[r] < y, parts[r][2], 0.0)
    top = functools.reduce(jnp.maximum, levels)
    top_before = functools.reduce(jnp.maximum, befores)
    whole = jnp.zeros((DK, DV), F32)
    early = jnp.zeros((DK, DV), F32)
    for r in range(4):
        whole = whole + jnp.exp(levels[r] - top) * parts[r][0]
        share = jnp.where(place[r] < y, jnp.exp(befores[r] - top_before), 0.0)
        early = early + share * parts[r][0]
    plane_ref[0:DK, :] = whole.astype(BF)
    plane_ref[DK:MSG, :] = scalar_tile(top, total_all)
    prefix_ref[0:DK, :] = early
    prefix_ref[DK : DK + 8, :] = jnp.broadcast_to(top_before, (8, DV))
    prefix_ref[DK + 8 : DK + 16, :] = jnp.broadcast_to(total_before, (8, DV))


def join_body(id_ref, near_ref, far_ref, out_ref):
    z, y = id_ref[0], id_ref[1]
    state_near, top_near, total_near = read_message(near_ref)
    state_far, top_far, total_far = read_message(far_ref)
    has_near = z >= 2 * y + 1
    has_far = (z >= 2 * y + 2) & (y < 3)
    top_near = jnp.where(has_near, top_near, LOWEST)
    total_near = jnp.where(has_near, total_near, 0.0)
    moved = jnp.where(has_far, top_far + total_near, LOWEST)
    total_far = jnp.where(has_far, total_far, 0.0)
    top = jnp.maximum(top_near, moved)
    share_near = jnp.where(has_near, jnp.exp(top_near - top), 0.0)
    share_far = jnp.where(has_far, jnp.exp(moved - top), 0.0)
    out_ref[0:DK, :] = (share_near * state_near + share_far * state_far).astype(BF)
    out_ref[DK:MSG, :] = scalar_tile(top, total_near + total_far)


def gated_body(
    id_ref, m0, m1, m2, m3, prefix_ref, num_ref, q_ref, a_ref, o_ref, gain_ref, res_ref, *outs
):
    y = id_ref[1]
    x = id_ref[2]
    c = id_ref[3]
    top_before = prefix_ref[DK : DK + 1, :]
    parts = [read_message(m) for m in (m0, m1, m2, m3)]
    place = [lax.rem(y - r + 4, 4) for r in range(4)]
    levels = []
    for r in range(4):
        level = parts[r][1] + prefix_ref[DK + 8 : DK + 9, :]
        for w in range(4):
            if w != r:
                level = level + jnp.where(place[w] < place[r], parts[w][2], 0.0)
        levels.append(level)
    top = functools.reduce(jnp.maximum, levels, top_before)
    carried = jnp.exp(top_before - top) * prefix_ref[0:DK, :]
    for r in range(4):
        carried = carried + jnp.exp(levels[r] - top) * parts[r][0]
    high = carried.astype(BF)
    gain = gain_ref[...].astype(F32)
    for r in (2, 1, 3, 0):
        for side, out in ((c, outs[r]), (1 - c, outs[4 + r])):
            group = side * 4 + lax.rem(x + r, 4)
            rows = pl.ds(pl.multiple_of(group * 128, 128), 128)
            line = jnp.broadcast_to(a_ref[1, pl.ds(group, 1), :], (128, 128))
            left = jnp.transpose(line)
            inner = jnp.concatenate([left, left], axis=1)
            row_max = jnp.maximum(inner, top)
            outer = jnp.dot(q_ref[rows, :], high, preferred_element_type=F32)
            memory = jnp.exp(inner - row_max) * num_ref[rows, :] + jnp.exp(top - row_max) * outer
            memory = memory * (DK**-0.5)
            mean = jnp.sum(memory * memory, axis=1, keepdims=True) * (1.0 / DV)
            normal = memory * lax.rsqrt(mean + EPSILON)
            opened = jax.nn.sigmoid(o_ref[rows, :].astype(F32))
            out[:, 0:256] = (normal * gain * opened).astype(BF)
            out[:, 256:512] = res_ref[rows, :]


def stream_body(id_ref, *refs):
    keeps, others, own_w, other_w = refs[0:4], refs[4:8], refs[8:12], refs[12:16]
    out_ref = refs[16]
    scratch = refs[17]
    x = id_ref[2]
    c = id_ref[3]
    for r in range(4):
        chip = lax.rem(x - r + 4, 4)
        scratch[chip * 2 + c] = keeps[r][:, 256:512]
        scratch[chip * 2 + 1 - c] = others[r][:, 256:512]
    for n in range(4):
        cols = slice(512 * n, 512 * (n + 1))
        total = jnp.concatenate(
            [scratch[2 * n].astype(F32), scratch[2 * n + 1].astype(F32)], axis=1
        )
        for r in range(4):
            total = total + jnp.dot(
                keeps[r][:, 0:256], own_w[r][:, cols], preferred_element_type=F32
            )
            total = total + jnp.dot(
                others[r][:, 0:256], other_w[r][:, cols], preferred_element_type=F32
            )
        out_ref[:, cols] = total.astype(BF)


def norm_body(id_ref, s0, s1, s2, s3, gain_ref, out_a, out_b, own_a, own_b, blocks):
    x = id_ref[2]
    for r, s in enumerate((s0, s1, s2, s3)):
        blocks[lax.rem(x - r + 4, 4)] = s[...]
    gain = gain_ref[...].astype(F32)
    cols = pl.ds(pl.multiple_of(x * 512, 512), 512)
    for k in range(4):
        out, own = ((out_a, own_a), (out_b, own_b))[k // 2]
        rows = slice(128 * (k % 2), 128 * (k % 2 + 1))
        wide = blocks[k].astype(F32)
        square = jnp.sum(wide * wide, axis=1, keepdims=True)
        scale = lax.rsqrt(square * (1.0 / 2048) + EPSILON)
        out[rows, :] = (wide * scale * gain).astype(BF)
        own[rows, :] = blocks[k, :, cols]


def feed_body(id_ref, n_ref, w_ref, o0, o1, o2, o3, weights, hidden, sems):
    x = id_ref[2]
    copies = {}
    for part in range(3):
        for side in range(2):
            copies[side, part] = pltpu.make_async_copy(
                w_ref.at[:, side, pl.ds(64 * part, 64), :],
                weights.at[side, part],
                sems.at[side, part],
            )
    for key in ((0, 0), (0, 1), (1, 0), (1, 1), (0, 2), (1, 2)):
        copies[key].start()
    for side in range(2):
        copies[side, 0].wait()
        gate = jnp.dot(
            n_ref[...], weights[side, 0].reshape(2048, FFD), preferred_element_type=F32
        )
        copies[side, 1].wait()
        up = jnp.dot(n_ref[...], weights[side, 1].reshape(2048, FFD), preferred_element_type=F32)
        hidden[side] = (gate * jax.nn.sigmoid(gate) * up).astype(BF)
    copies[0, 2].wait()
    copies[1, 2].wait()
    for r, out in ((2, o2), (1, o1), (3, o3), (0, o0)):
        begin = lax.rem(x + r, 4) * 8
        total = jnp.zeros((PART, HALF), F32)
        for side in range(2):
            block = weights[side, 2, pl.ds(begin, 8)].reshape(512, FFD)
            total = total + lax.dot_general(
                hidden[side], block, (((1,), (1,)), ((), ())), preferred_element_type=F32
            )
        out[...] = total.astype(BF)


def mixed_halves(id_ref, stream_ref, parts):
    c = id_ref[3]
    total = sum(p[...].astype(F32) for p in parts)
    mixed = (stream_ref[...].astype(F32) + 0.5 * total).astype(BF)
    left, right = mixed[:, 0:256], mixed[:, 256:512]
    return jnp.where(c == 0, left, right), jnp.where(c == 0, right, left)


def mix_a_body(id_ref, stream_ref, p0, p1, p2, p3, mine_ref, send_ref):
    mine_ref[...], send_ref[...] = mixed_halves(id_ref, stream_ref, (p0, p1, p2, p3))


def mix_b_body(id_ref, stream_ref, p0, p1, p2, p3, mine_a, theirs_a, whole_ref, send_ref):
    c = id_ref[3]
    mine, send_ref[...] = mixed_halves(id_ref, stream_ref, (p0, p1, p2, p3))
    own = pl.multiple_of(c * HALF, PART)
    other = pl.multiple_of((1 - c) * HALF, PART)
    whole_ref[pl.ds(own, PART), :] = mine_a[...]
    whole_ref[pl.ds(own + PART, PART), :] = mine
    whole_ref[pl.ds(other, PART), :] = theirs_a[...]
    whole_ref[pl.ds(other + PART, PART), :] = mine


def shift(array, axis, count, by):
    return lax.ppermute(array, axis, [(i, (i + by) % count) for i in range(count)])


def column(array, steps):
    pairs = []
    for y in range(4):
        for z in range(8 - steps[y]):
            pairs.append((4 * z + y, 4 * (z + steps[y]) + y))
    return lax.ppermute(array, SP, pairs)


def swap(array):
    return lax.ppermute(array, "c", [(0, 1), (1, 0)])


def cross(array, by):
    pairs = []
    for i in range(4):
        for j in range(2):
            pairs.append((2 * i + j, 2 * ((i + by) % 4) + 1 - j))
    return lax.ppermute(array, TP, pairs)


def spread(array, axis):
    return [array] + [shift(array, axis, 4, r) for r in (1, 2, 3)]


def layer(
    queries,
    cell_key_rows,
    cell_value_rows,
    output_gate_logits,
    input_gate_logits,
    forget_gate_logits,
    forget_extra_term,
    residual,
    head_norm_gain,
    cell_output_weight,
    feedforward_norm_gain,
    gate_projection_weight,
    up_projection_weight,
    down_projection_weight,
):
    z, y, x, c = (lax.axis_index(n) for n in ("z", "y", "x", "c"))
    place = jnp.stack([z, y, x, c]).astype(jnp.int32)

    own_out = spread(cell_output_weight, "x")
    other_out = [swap(rows) for rows in own_out]

    message, levels = call(
        summary_body,
        (shape((MSG, DV)), shape((2, 8, 128), F32)),
        (cell_key_rows, cell_value_rows, input_gate_logits, forget_gate_logits, forget_extra_term),
        vmem=60,
    )
    near = spread(message, "y")[1:]

    shard = jnp.concatenate(
        [gate_projection_weight, up_projection_weight, down_projection_weight.T], axis=0
    )
    weights = lax.all_gather(shard, ("z", "y", "c")).reshape(32, 2, 192, FFD)

    numerator = call(
        inside_body,
        shape((ROWS, DV), F32),
        (queries, cell_key_rows, cell_value_rows, levels),
        flops=2000000000,
        vmem=60,
    )
    plane, prefix = call(
        plane_body,
        (shape((MSG, DV)), shape((MSG, DV), F32)),
        (place, message, *near),
        in_specs=[SMEM] + [VMEM] * 4,
    )
    joined = call(
        join_body,
        shape((MSG, DV)),
        (place, column(plane, (1, 3, 5, 7)), column(plane, (2, 4, 6, 8))),
        in_specs=[SMEM] + [VMEM] * 2,
    )
    gated = call(
        gated_body,
        tuple(shape((128, 512)) for _ in range(8)),
        (place, *spread(joined, "y"), prefix, numerator, queries, levels,
         output_gate_logits, head_norm_gain.reshape(1, DV), residual),
        in_specs=[SMEM] + [VMEM] * 11,
        vmem=60,
    )
    keeps = [gated[0]] + [shift(gated[r], "x", 4, r) for r in (1, 2, 3)]
    others = [cross(gated[4 + r], r) for r in range(4)]
    stream = call(
        stream_body,
        shape((128, 2048)),
        (place, *keeps, *others, *own_out, *other_out),
        in_specs=[SMEM] + [VMEM] * 16,
        scratch=(pltpu.VMEM((8, 128, 256), BF),),
        vmem=20,
    )
    streams = spread(stream, "x")
    normed_a, normed_b, own_a, own_b = call(
        norm_body,
        (shape((PART, 2048)), shape((PART, 2048)), shape((PART, HALF)), shape((PART, HALF))),
        (place, *streams, feedforward_norm_gain.reshape(1, 2048)),
        in_specs=[SMEM] + [VMEM] * 5,
        scratch=(pltpu.VMEM((4, 128, 2048), BF),),
    )

    def feed(normed):
        parts = call(
            feed_body,
            tuple(shape((PART, HALF)) for _ in range(4)),
            (place, normed, weights),
            in_specs=[SMEM, VMEM, ANY],
            scratch=(
                pltpu.VMEM((2, 3, 32, 64, FFD), BF),
                pltpu.VMEM((2, PART, FFD), BF),
                pltpu.SemaphoreType.DMA((2, 3)),
            ),
            flops=4500000000,
            vmem=36,
        )
        return [parts[0]] + [shift(parts[r], "x", 4, r) for r in (1, 2, 3)]

    arrived_a = feed(normed_a)
    arrived_b = feed(normed_b)
    mine_a, theirs_a = call(
        mix_a_body,
        (shape((PART, 256)), shape((PART, 256))),
        (place, own_a, *arrived_a),
        in_specs=[SMEM] + [VMEM] * 5,
    )
    whole, theirs_b = call(
        mix_b_body,
        (shape((ROWS, 256)), shape((PART, 256))),
        (place, own_b, *arrived_b, mine_a, swap(theirs_a)),
        in_specs=[SMEM] + [VMEM] * 7,
    )
    return lax.dynamic_update_slice(whole, swap(theirs_b), ((1 - c) * HALF + PART, jnp.int32(0)))


def solution(mesh):
    torus = Mesh(mesh.devices.reshape(8, 4, 4, 2), ("z", "y", "x", "c"))
    in_specs = (
        P(SP, TP),
        P(SP, TP),
        P(SP, TP),
        P(SP, TP),
        P(TP, SP),
        P(TP, SP),
        P(TP, SP),
        P(SP, TP),
        P(TP),
        P(TP, None),
        P(),
        P(SP, TP),
        P(SP, TP),
        P(TP, SP),
    )
    out_specs = P(SP, TP)
    return jax.shard_map(layer, mesh=torus, in_specs=in_specs, out_specs=out_specs, check_vma=False)
```

```python
import functools

import jax
import jax.numpy as jnp
from jax import lax
from jax.experimental import pallas as pl
from jax.experimental.pallas import tpu as pltpu
from jax.sharding import Mesh
from jax.sharding import PartitionSpec as P


SP = ("z", "y")
TP = ("x", "c")
BF = jnp.bfloat16
F32 = jnp.float32
LOWEST = -1e30
EPSILON = 1e-06
ROWS = 1024
HALF = 512
PART = 256
DK = 128
DV = 256
MSG = 144
FFD = 704
FEED_VMEM = 20

VMEM = pl.BlockSpec(memory_space=pltpu.VMEM)
SMEM = pl.BlockSpec(memory_space=pltpu.SMEM)
ANY = pl.BlockSpec(memory_space=pltpu.HBM)


def call(body, outs, ins, scratch=(), flops=1000000, in_specs=None, vmem=12):
    return pl.pallas_call(
        body,
        out_shape=outs,
        in_specs=in_specs or [VMEM] * len(ins),
        out_specs=jax.tree.map(lambda _: VMEM, outs),
        scratch_shapes=list(scratch),
        cost_estimate=pl.CostEstimate(flops=flops, bytes_accessed=1000000, transcendentals=0),
        compiler_params=pltpu.CompilerParams(vmem_limit_bytes=vmem * 1024 * 1024),
    )(*ins)


def shape(dims, dtype=BF):
    return jax.ShapeDtypeStruct(dims, dtype)


def scan_rows(values, combine, fill):
    lane = lax.broadcasted_iota(jnp.int32, (8, 128), 1)
    row = lax.broadcasted_iota(jnp.int32, (8, 128), 0)
    for step in (1, 2, 4, 8, 16, 32, 64):
        moved = pltpu.roll(values, step, 1)
        values = combine(values, jnp.where(lane >= step, moved, fill))
    last = jnp.broadcast_to(values[:, 127:128], (8, 128))
    before = jnp.where(row >= 1, pltpu.roll(last, 1, 0), fill)
    for step in (1, 2, 4):
        moved = pltpu.roll(before, step, 0)
        before = combine(before, jnp.where(row >= step, moved, fill))
    return combine(values, before)


def eight_rows(ref):
    wide = ref[...].astype(F32)
    return jnp.concatenate([wide[:, 128 * k : 128 * (k + 1)] for k in range(8)], axis=0)


def as_column(values, k):
    return jnp.transpose(jnp.broadcast_to(values[k : k + 1, :], (128, 128)))


def split3(value):
    high = value.astype(BF).astype(F32)
    middle = (value - high).astype(BF).astype(F32)
    return high, middle, value - high - middle


def scalar_tile(top, total, width=256):
    row = lax.broadcasted_iota(jnp.int32, (16, width), 0)
    tile = jnp.zeros((16, width), F32)
    for k, part in enumerate(split3(top) + split3(total)):
        tile = jnp.where(row == k, jnp.broadcast_to(part, (16, width)), tile)
    return tile.astype(BF)


def read_message(ref):
    tile = ref[DK:MSG, :].astype(F32)
    top = tile[0:1] + tile[1:2] + tile[2:3]
    total = tile[3:4] + tile[4:5] + tile[5:6]
    return ref[0:DK, :].astype(F32), top, total


def summary_body(k_ref, v_ref, ig_ref, fg_ref, fe_ref, msg_ref, a_ref):
    gate = eight_rows(ig_ref)
    forget = eight_rows(fg_ref)
    extra = eight_rows(fe_ref)
    small = jnp.exp(-jnp.abs(forget))
    series = small * (1.0 - small * (0.5 - small * (1 / 3 - small * (0.25 - small * 0.2))))
    log_one = jnp.where(small < 0.03, series, jnp.log(1.0 + small))
    log_forget = jnp.minimum(forget, 0.0) - log_one + extra
    running = scan_rows(log_forget, jnp.add, 0.0)
    level = gate - running
    highest = scan_rows(level, jnp.maximum, LOWEST)
    a_ref[0] = level
    a_ref[1] = highest
    final = jnp.broadcast_to(highest[7:8, 127:128], (8, 128))
    weight = jnp.exp(level - final)
    total = jnp.zeros((DK, DV), F32)
    for b in range(8):
        rows = slice(128 * b, 128 * (b + 1))
        scaled = (k_ref[rows, :].astype(F32) * as_column(weight, b)).astype(BF)
        total = total + lax.dot_general(
            scaled, v_ref[rows, :], (((0,), (0,)), ((), ())), preferred_element_type=F32
        )
    msg_ref[0:DK, :] = total.astype(BF)
    all_forget = running[7:8, 127:128]
    msg_ref[DK:MSG, :] = scalar_tile(highest[7:8, 127:128] + all_forget, all_forget)


def inside_body(q_ref, k_ref, v_ref, a_ref, num_ref):
    level = a_ref[0]
    highest = a_ref[1]
    t = lax.broadcasted_iota(jnp.int32, (256, 256), 0)
    s = lax.broadcasted_iota(jnp.int32, (256, 256), 1)
    causal = t >= s
    for i in range(4):
        left = jnp.concatenate([as_column(highest, 2 * i), as_column(highest, 2 * i + 1)], axis=0)
        column = jnp.concatenate([left, left], axis=1)
        query = q_ref[256 * i : 256 * (i + 1), :]
        total = jnp.zeros((256, DV), F32)
        for j in range(i + 1):
            rows = slice(256 * j, 256 * (j + 1))
            line = jnp.concatenate([level[2 * j : 2 * j + 1], level[2 * j + 1 : 2 * j + 2]], axis=1)
            score = lax.dot_general(
                query, k_ref[rows, :], (((1,), (1,)), ((), ())), preferred_element_type=F32
            )
            weight = jnp.exp(line - column)
            if i == j:
                weight = jnp.where(causal, weight, 0.0)
            total = total + jnp.dot(
                (score * weight).astype(BF), v_ref[rows, :], preferred_element_type=F32
            )
        num_ref[256 * i : 256 * (i + 1), :] = total


def plane_body(m0, m1, m2, m3, plane_ref, prefix_ref):
    y = lax.axis_index("y")
    parts = [read_message(m) for m in (m0, m1, m2, m3)]
    place = [lax.rem(y - r + 4, 4) for r in range(4)]
    levels, befores = [], []
    total_all = jnp.zeros((1, DV), F32)
    total_before = jnp.zeros((1, DV), F32)
    for r in range(4):
        level = parts[r][1]
        before = parts[r][1]
        for w in range(4):
            if w != r:
                later = place[w] > place[r]
                level = level + jnp.where(later, parts[w][2], 0.0)
                before = before + jnp.where(later & (place[w] < y), parts[w][2], 0.0)
        levels.append(level)
        befores.append(jnp.where(place[r] < y, before, LOWEST))
        total_all = total_all + parts[r][2]
        total_before = total_before + jnp.where(place[r] < y, parts[r][2], 0.0)
    top = functools.reduce(jnp.maximum, levels)
    top_before = functools.reduce(jnp.maximum, befores)
    whole = jnp.zeros((DK, DV), F32)
    early = jnp.zeros((DK, DV), F32)
    for r in range(4):
        whole = whole + jnp.exp(levels[r] - top) * parts[r][0]
        share = jnp.where(place[r] < y, jnp.exp(befores[r] - top_before), 0.0)
        early = early + share * parts[r][0]
    plane_ref[0:DK, :] = whole.astype(BF)
    plane_ref[DK:MSG, :] = scalar_tile(top, total_all)
    prefix_ref[0:DK, :] = early
    prefix_ref[DK : DK + 8, :] = jnp.broadcast_to(top_before, (8, DV))
    prefix_ref[DK + 8 : DK + 16, :] = jnp.broadcast_to(total_before, (8, DV))


def join_body(near_ref, far_ref, out_ref):
    z, y = lax.axis_index("z"), lax.axis_index("y")
    state_near, top_near, total_near = read_message(near_ref)
    state_far, top_far, total_far = read_message(far_ref)
    has_near = z >= 2 * y + 1
    has_far = (z >= 2 * y + 2) & (y < 3)
    top_near = jnp.where(has_near, top_near, LOWEST)
    total_near = jnp.where(has_near, total_near, 0.0)
    moved = jnp.where(has_far, top_far + total_near, LOWEST)
    total_far = jnp.where(has_far, total_far, 0.0)
    top = jnp.maximum(top_near, moved)
    share_near = jnp.where(has_near, jnp.exp(top_near - top), 0.0)
    share_far = jnp.where(has_far, jnp.exp(moved - top), 0.0)
    out_ref[0:DK, :] = (share_near * state_near + share_far * state_far).astype(BF)
    out_ref[DK:MSG, :] = scalar_tile(top, total_near + total_far)


def gated_body(
    m0, m1, m2, m3, prefix_ref, num_ref, q_ref, a_ref, o_ref, gain_ref, res_ref, *outs
):
    y = lax.axis_index("y")
    x = lax.axis_index("x")
    c = lax.axis_index("c")
    top_before = prefix_ref[DK : DK + 1, :]
    parts = [read_message(m) for m in (m0, m1, m2, m3)]
    place = [lax.rem(y - r + 4, 4) for r in range(4)]
    levels = []
    for r in range(4):
        level = parts[r][1] + prefix_ref[DK + 8 : DK + 9, :]
        for w in range(4):
            if w != r:
                level = level + jnp.where(place[w] < place[r], parts[w][2], 0.0)
        levels.append(level)
    top = functools.reduce(jnp.maximum, levels, top_before)
    carried = jnp.exp(top_before - top) * prefix_ref[0:DK, :]
    for r in range(4):
        carried = carried + jnp.exp(levels[r] - top) * parts[r][0]
    high = carried.astype(BF)
    gain = gain_ref[...].astype(F32)
    for r in (2, 1, 3, 0):
        for side, out in ((c, outs[r]), (1 - c, outs[4 + r])):
            group = side * 4 + lax.rem(x + r, 4)
            rows = pl.ds(pl.multiple_of(group * 128, 128), 128)
            line = jnp.broadcast_to(a_ref[1, pl.ds(group, 1), :], (128, 128))
            left = jnp.transpose(line)
            inner = jnp.concatenate([left, left], axis=1)
            row_max = jnp.maximum(inner, top)
            outer = jnp.dot(q_ref[rows, :], high, preferred_element_type=F32)
            memory = jnp.exp(inner - row_max) * num_ref[rows, :] + jnp.exp(top - row_max) * outer
            memory = memory * (DK**-0.5)
            mean = jnp.sum(memory * memory, axis=1, keepdims=True) * (1.0 / DV)
            normal = memory * lax.rsqrt(mean + EPSILON)
            opened = jax.nn.sigmoid(o_ref[rows, :].astype(F32))
            out[:, 0:256] = (normal * gain * opened).astype(BF)
            out[:, 256:512] = res_ref[rows, :]


def stream_body(*refs):
    keeps, others, own_w, other_w = refs[0:4], refs[4:8], refs[8:12], refs[12:16]
    out_ref, scratch = refs[16:18]
    x = lax.axis_index("x")
    c = lax.axis_index("c")
    for r in range(4):
        chip = lax.rem(x - r + 4, 4)
        scratch[chip * 2 + c] = keeps[r][:, 256:512]
        scratch[chip * 2 + 1 - c] = others[r][:, 256:512]

    def columns(n, carry):
        cols = pl.ds(pl.multiple_of(512 * n, 512), 512)
        total = jnp.concatenate(
            [scratch[2 * n].astype(F32), scratch[2 * n + 1].astype(F32)], axis=1
        )
        for r in range(4):
            total = total + jnp.dot(
                keeps[r][:, 0:256], own_w[r][:, cols], preferred_element_type=F32
            )
            total = total + jnp.dot(
                others[r][:, 0:256], other_w[r][:, cols], preferred_element_type=F32
            )
        out_ref[:, cols] = total.astype(BF)
        return carry

    lax.fori_loop(0, 4, columns, 0)


def norm_body(s0, s1, s2, s3, gain_ref, out_a, out_b, own_a, own_b, blocks):
    x = lax.axis_index("x")
    for r, s in enumerate((s0, s1, s2, s3)):
        blocks[lax.rem(x - r + 4, 4)] = s[...]
    gain = gain_ref[...].astype(F32)
    cols = pl.ds(pl.multiple_of(x * 512, 512), 512)
    for k in range(4):
        out, own = ((out_a, own_a), (out_b, own_b))[k // 2]
        rows = slice(128 * (k % 2), 128 * (k % 2 + 1))
        wide = blocks[k].astype(F32)
        square = jnp.sum(wide * wide, axis=1, keepdims=True)
        scale = lax.rsqrt(square * (1.0 / 2048) + EPSILON)
        out[rows, :] = (wide * scale * gain).astype(BF)
        own[rows, :] = blocks[k, :, cols]


def feed_ordered(n_ref, weights, hidden, wait, outs):
    x = lax.axis_index("x")

    def open_side(side, carry):
        wait(side, 0)
        gate = jnp.dot(
            n_ref[...], weights[side, 0].reshape(2048, FFD), preferred_element_type=F32
        )
        wait(side, 1)
        up = jnp.dot(n_ref[...], weights[side, 1].reshape(2048, FFD), preferred_element_type=F32)
        hidden[side] = (gate * jax.nn.sigmoid(gate) * up).astype(BF)
        return carry

    lax.fori_loop(0, 2, open_side, 0)
    for side in range(2):
        wait(side, 2)
    for r in (1, 3, 2, 0):
        begin = lax.rem(x + r, 4) * 8
        total = jnp.zeros((PART, HALF), F32)
        for side in range(2):
            block = weights[side, 2, pl.ds(begin, 8)].reshape(512, FFD)
            total = total + lax.dot_general(
                hidden[side], block, (((1,), (1,)), ((), ())), preferred_element_type=F32
            )
        outs[r][...] = total.astype(BF)


def feed_a_body(n_ref, w_ref, o0, o1, o2, o3, weights, hidden, sems):
    def copy(side, part):
        return pltpu.make_async_copy(
            w_ref.at[:, side, pl.ds(64 * part, 64), :],
            weights.at[side, part],
            sems.at[side, part],
        )

    for side, part in ((0, 0), (0, 1), (1, 0), (1, 1), (0, 2), (1, 2)):
        copy(side, part).start()
    feed_ordered(
        n_ref, weights, hidden, lambda side, part: copy(side, part).wait(), (o0, o1, o2, o3)
    )


def feed_b_body(n_ref, weights, o0, o1, o2, o3, hidden):
    feed_ordered(n_ref, weights, hidden, lambda side, part: None, (o0, o1, o2, o3))


def mixed_halves(stream_ref, parts):
    c = lax.axis_index("c")
    total = sum(p[...].astype(F32) for p in parts)
    mixed = (stream_ref[...].astype(F32) + 0.5 * total).astype(BF)
    left, right = mixed[:, 0:256], mixed[:, 256:512]
    return jnp.where(c == 0, left, right), jnp.where(c == 0, right, left)


def mix_a_body(stream_ref, p0, p1, p2, p3, mine_ref, send_ref):
    mine_ref[...], send_ref[...] = mixed_halves(stream_ref, (p0, p1, p2, p3))


def mix_b_body(stream_ref, p0, p1, p2, p3, mine_a, theirs_a, whole_ref, send_ref):
    c = lax.axis_index("c")
    mine, send_ref[...] = mixed_halves(stream_ref, (p0, p1, p2, p3))
    own = pl.multiple_of(c * HALF, PART)
    other = pl.multiple_of((1 - c) * HALF, PART)
    whole_ref[pl.ds(own, PART), :] = mine_a[...]
    whole_ref[pl.ds(own + PART, PART), :] = mine
    whole_ref[pl.ds(other, PART), :] = theirs_a[...]
    whole_ref[pl.ds(other + PART, PART), :] = mine


def shift(array, axis, count, by):
    return lax.ppermute(array, axis, [(i, (i + by) % count) for i in range(count)])


def column(array, steps):
    pairs = []
    for y in range(4):
        for z in range(8 - steps[y]):
            pairs.append((4 * z + y, 4 * (z + steps[y]) + y))
    return lax.ppermute(array, SP, pairs)


def swap(array):
    return lax.ppermute(array, "c", [(0, 1), (1, 0)])


def cross(array, by):
    pairs = []
    for i in range(4):
        for j in range(2):
            pairs.append((2 * i + j, 2 * ((i + by) % 4) + 1 - j))
    return lax.ppermute(array, TP, pairs)


def spread(array, axis):
    return [array] + [shift(array, axis, 4, r) for r in (1, 2, 3)]


def layer(
    queries,
    cell_key_rows,
    cell_value_rows,
    output_gate_logits,
    input_gate_logits,
    forget_gate_logits,
    forget_extra_term,
    residual,
    head_norm_gain,
    cell_output_weight,
    feedforward_norm_gain,
    gate_projection_weight,
    up_projection_weight,
    down_projection_weight,
):
    c = lax.axis_index("c")

    own_out = spread(cell_output_weight, "x")
    other_out = [swap(rows) for rows in own_out]

    message, levels = call(
        summary_body,
        (shape((MSG, DV)), shape((2, 8, 128), F32)),
        (cell_key_rows, cell_value_rows, input_gate_logits, forget_gate_logits, forget_extra_term),
        vmem=60,
    )
    near = spread(message, "y")[1:]

    shard = jnp.concatenate(
        [gate_projection_weight, up_projection_weight, down_projection_weight.T], axis=0
    )
    weights = lax.all_gather(shard, ("z", "y", "c")).reshape(32, 2, 192, FFD)

    numerator = call(
        inside_body,
        shape((ROWS, DV), F32),
        (queries, cell_key_rows, cell_value_rows, levels),
        flops=2000000000,
        vmem=60,
    )
    plane, prefix = call(
        plane_body, (shape((MSG, DV)), shape((MSG, DV), F32)), (message, *near), in_specs=[VMEM] * 4
    )
    joined = call(
        join_body,
        shape((MSG, DV)),
        (column(plane, (1, 3, 5, 7)), column(plane, (2, 4, 6, 8))),
        in_specs=[VMEM] * 2,
    )
    gated = call(
        gated_body,
        tuple(shape((128, 512)) for _ in range(8)),
        (*spread(joined, "y"), prefix, numerator, queries, levels,
         output_gate_logits, head_norm_gain.reshape(1, DV), residual),
        in_specs=[VMEM] * 11,
        vmem=60,
    )
    keeps = [gated[0]] + [shift(gated[r], "x", 4, r) for r in (1, 2, 3)]
    others = [cross(gated[4 + r], r) for r in range(4)]
    stream = call(
        stream_body,
        shape((128, 2048)),
        (*keeps, *others, *own_out, *other_out),
        in_specs=[VMEM] * 16,
        scratch=(pltpu.VMEM((8, 128, 256), BF),),
        vmem=20,
    )
    streams = spread(stream, "x")
    normed_a, normed_b, own_a, own_b = call(
        norm_body,
        (shape((PART, 2048)), shape((PART, 2048)), shape((PART, HALF)), shape((PART, HALF))),
        (*streams, feedforward_norm_gain.reshape(1, 2048)),
        in_specs=[VMEM] * 5,
        scratch=(pltpu.VMEM((4, 128, 2048), BF),),
    )

    def exchanged(parts):
        return [parts[0]] + [shift(parts[r], "x", 4, r) for r in (1, 2, 3)]

    *parts_a, resident = call(
        feed_a_body,
        tuple(shape((PART, HALF)) for _ in range(4)) + (shape((2, 3, 32, 64, FFD)),),
        (normed_a, weights),
        in_specs=[VMEM, ANY],
        scratch=(pltpu.VMEM((2, PART, FFD), BF), pltpu.SemaphoreType.DMA((2, 3))),
        flops=4500000000,
        vmem=FEED_VMEM,
    )
    parts_b = call(
        feed_b_body,
        tuple(shape((PART, HALF)) for _ in range(4)),
        (normed_b, resident),
        scratch=(pltpu.VMEM((2, PART, FFD), BF),),
        flops=4500000000,
        vmem=FEED_VMEM,
    )
    arrived_a = exchanged(parts_a)
    arrived_b = exchanged(parts_b)
    mine_a, theirs_a = call(
        mix_a_body,
        (shape((PART, 256)), shape((PART, 256))),
        (own_a, *arrived_a),
        in_specs=[VMEM] * 5,
    )
    whole, theirs_b = call(
        mix_b_body,
        (shape((ROWS, 256)), shape((PART, 256))),
        (own_b, *arrived_b, mine_a, swap(theirs_a)),
        in_specs=[VMEM] * 7,
    )
    return lax.dynamic_update_slice(whole, swap(theirs_b), ((1 - c) * HALF + PART, jnp.int32(0)))


def solution(mesh):
    torus = Mesh(mesh.devices.reshape(8, 4, 4, 2), ("z", "y", "x", "c"))
    in_specs = (
        P(SP, TP),
        P(SP, TP),
        P(SP, TP),
        P(SP, TP),
        P(TP, SP),
        P(TP, SP),
        P(TP, SP),
        P(SP, TP),
        P(TP),
        P(TP, None),
        P(),
        P(SP, TP),
        P(SP, TP),
        P(TP, SP),
    )
    out_specs = P(SP, TP)
    return jax.shard_map(layer, mesh=torus, in_specs=in_specs, out_specs=out_specs, check_vma=False)
```

```python
import functools

import jax
import jax.numpy as jnp
from jax import lax
from jax.experimental import pallas as pl
from jax.experimental.pallas import tpu as pltpu
from jax.sharding import Mesh
from jax.sharding import PartitionSpec as P


SP = ("z", "y")
TP = ("x", "c")
BF = jnp.bfloat16
F32 = jnp.float32
LOWEST = -1e30
EPSILON = 1e-06
ROWS = 1024
HALF = 512
PART = 256
DK = 128
DV = 256
MSG = 144
FFD = 704
FEED_VMEM = 20

VMEM = pl.BlockSpec(memory_space=pltpu.VMEM)
SMEM = pl.BlockSpec(memory_space=pltpu.SMEM)
ANY = pl.BlockSpec(memory_space=pltpu.HBM)


def call(body, outs, ins, scratch=(), flops=1000000, in_specs=None, vmem=12):
    return pl.pallas_call(
        body,
        out_shape=outs,
        in_specs=in_specs or [VMEM] * len(ins),
        out_specs=jax.tree.map(lambda _: VMEM, outs),
        scratch_shapes=list(scratch),
        cost_estimate=pl.CostEstimate(flops=flops, bytes_accessed=1000000, transcendentals=0),
        compiler_params=pltpu.CompilerParams(vmem_limit_bytes=vmem * 1024 * 1024),
    )(*ins)


def shape(dims, dtype=BF):
    return jax.ShapeDtypeStruct(dims, dtype)


def scan_rows(values, combine, fill):
    lane = lax.broadcasted_iota(jnp.int32, (8, 128), 1)
    row = lax.broadcasted_iota(jnp.int32, (8, 128), 0)
    for step in (1, 2, 4, 8, 16, 32, 64):
        moved = pltpu.roll(values, step, 1)
        values = combine(values, jnp.where(lane >= step, moved, fill))
    last = jnp.broadcast_to(values[:, 127:128], (8, 128))
    before = jnp.where(row >= 1, pltpu.roll(last, 1, 0), fill)
    for step in (1, 2, 4):
        moved = pltpu.roll(before, step, 0)
        before = combine(before, jnp.where(row >= step, moved, fill))
    return combine(values, before)


def eight_rows(ref):
    wide = ref[...].astype(F32)
    return jnp.concatenate([wide[:, 128 * k : 128 * (k + 1)] for k in range(8)], axis=0)


def as_column(values, k):
    return jnp.transpose(jnp.broadcast_to(values[k : k + 1, :], (128, 128)))


def split3(value):
    high = value.astype(BF).astype(F32)
    middle = (value - high).astype(BF).astype(F32)
    return high, middle, value - high - middle


def scalar_tile(top, total, width=256):
    row = lax.broadcasted_iota(jnp.int32, (16, width), 0)
    tile = jnp.zeros((16, width), F32)
    for k, part in enumerate(split3(top) + split3(total)):
        tile = jnp.where(row == k, jnp.broadcast_to(part, (16, width)), tile)
    return tile.astype(BF)


def read_message(ref):
    tile = ref[DK:MSG, :].astype(F32)
    top = tile[0:1] + tile[1:2] + tile[2:3]
    total = tile[3:4] + tile[4:5] + tile[5:6]
    return ref[0:DK, :].astype(F32), top, total


def summary_body(k_ref, v_ref, ig_ref, fg_ref, fe_ref, msg_ref, a_ref):
    gate = eight_rows(ig_ref)
    forget = eight_rows(fg_ref)
    extra = eight_rows(fe_ref)
    small = jnp.exp(-jnp.abs(forget))
    series = small * (1.0 - small * (0.5 - small * (1 / 3 - small * (0.25 - small * 0.2))))
    log_one = jnp.where(small < 0.03, series, jnp.log(1.0 + small))
    log_forget = jnp.minimum(forget, 0.0) - log_one + extra
    running = scan_rows(log_forget, jnp.add, 0.0)
    level = gate - running
    highest = scan_rows(level, jnp.maximum, LOWEST)
    a_ref[0] = level
    a_ref[1] = highest
    final = jnp.broadcast_to(highest[7:8, 127:128], (8, 128))
    weight = jnp.exp(level - final)
    total = jnp.zeros((DK, DV), F32)
    for b in range(8):
        rows = slice(128 * b, 128 * (b + 1))
        scaled = (k_ref[rows, :].astype(F32) * as_column(weight, b)).astype(BF)
        total = total + lax.dot_general(
            scaled, v_ref[rows, :], (((0,), (0,)), ((), ())), preferred_element_type=F32
        )
    msg_ref[0:DK, :] = total.astype(BF)
    all_forget = running[7:8, 127:128]
    msg_ref[DK:MSG, :] = scalar_tile(highest[7:8, 127:128] + all_forget, all_forget)


def inside_body(q_ref, k_ref, v_ref, a_ref, num_ref):
    level = a_ref[0]
    highest = a_ref[1]
    t = lax.broadcasted_iota(jnp.int32, (256, 256), 0)
    s = lax.broadcasted_iota(jnp.int32, (256, 256), 1)
    causal = t >= s
    for i in range(4):
        left = jnp.concatenate([as_column(highest, 2 * i), as_column(highest, 2 * i + 1)], axis=0)
        column = jnp.concatenate([left, left], axis=1)
        query = q_ref[256 * i : 256 * (i + 1), :]
        total = jnp.zeros((256, DV), F32)
        for j in range(i + 1):
            rows = slice(256 * j, 256 * (j + 1))
            line = jnp.concatenate([level[2 * j : 2 * j + 1], level[2 * j + 1 : 2 * j + 2]], axis=1)
            score = lax.dot_general(
                query, k_ref[rows, :], (((1,), (1,)), ((), ())), preferred_element_type=F32
            )
            weight = jnp.exp(line - column)
            if i == j:
                weight = jnp.where(causal, weight, 0.0)
            total = total + jnp.dot(
                (score * weight).astype(BF), v_ref[rows, :], preferred_element_type=F32
            )
        num_ref[256 * i : 256 * (i + 1), :] = total


def plane_body(m0, m1, m2, m3, plane_ref, prefix_ref):
    y = lax.axis_index("y")
    parts = [read_message(m) for m in (m0, m1, m2, m3)]
    place = [lax.rem(y - r + 4, 4) for r in range(4)]
    levels, befores = [], []
    total_all = jnp.zeros((1, DV), F32)
    total_before = jnp.zeros((1, DV), F32)
    for r in range(4):
        level = parts[r][1]
        before = parts[r][1]
        for w in range(4):
            if w != r:
                later = place[w] > place[r]
                level = level + jnp.where(later, parts[w][2], 0.0)
                before = before + jnp.where(later & (place[w] < y), parts[w][2], 0.0)
        levels.append(level)
        befores.append(jnp.where(place[r] < y, before, LOWEST))
        total_all = total_all + parts[r][2]
        total_before = total_before + jnp.where(place[r] < y, parts[r][2], 0.0)
    top = functools.reduce(jnp.maximum, levels)
    top_before = functools.reduce(jnp.maximum, befores)
    whole = jnp.zeros((DK, DV), F32)
    early = jnp.zeros((DK, DV), F32)
    for r in range(4):
        whole = whole + jnp.exp(levels[r] - top) * parts[r][0]
        share = jnp.where(place[r] < y, jnp.exp(befores[r] - top_before), 0.0)
        early = early + share * parts[r][0]
    plane_ref[0:DK, :] = whole.astype(BF)
    plane_ref[DK:MSG, :] = scalar_tile(top, total_all)
    prefix_ref[0:DK, :] = early
    prefix_ref[DK : DK + 8, :] = jnp.broadcast_to(top_before, (8, DV))
    prefix_ref[DK + 8 : DK + 16, :] = jnp.broadcast_to(total_before, (8, DV))


def join_body(near_ref, far_ref, out_ref):
    z, y = lax.axis_index("z"), lax.axis_index("y")
    state_near, top_near, total_near = read_message(near_ref)
    state_far, top_far, total_far = read_message(far_ref)
    has_near = z >= 2 * y + 1
    has_far = (z >= 2 * y + 2) & (y < 3)
    top_near = jnp.where(has_near, top_near, LOWEST)
    total_near = jnp.where(has_near, total_near, 0.0)
    moved = jnp.where(has_far, top_far + total_near, LOWEST)
    total_far = jnp.where(has_far, total_far, 0.0)
    top = jnp.maximum(top_near, moved)
    share_near = jnp.where(has_near, jnp.exp(top_near - top), 0.0)
    share_far = jnp.where(has_far, jnp.exp(moved - top), 0.0)
    out_ref[0:DK, :] = (share_near * state_near + share_far * state_far).astype(BF)
    out_ref[DK:MSG, :] = scalar_tile(top, total_near + total_far)


def gated_body(
    m0, m1, m2, m3, prefix_ref, num_ref, q_ref, a_ref, o_ref, gain_ref, res_ref, *outs
):
    y = lax.axis_index("y")
    x = lax.axis_index("x")
    c = lax.axis_index("c")
    top_before = prefix_ref[DK : DK + 1, :]
    parts = [read_message(m) for m in (m0, m1, m2, m3)]
    place = [lax.rem(y - r + 4, 4) for r in range(4)]
    levels = []
    for r in range(4):
        level = parts[r][1] + prefix_ref[DK + 8 : DK + 9, :]
        for w in range(4):
            if w != r:
                level = level + jnp.where(place[w] < place[r], parts[w][2], 0.0)
        levels.append(level)
    top = functools.reduce(jnp.maximum, levels, top_before)
    carried = jnp.exp(top_before - top) * prefix_ref[0:DK, :]
    for r in range(4):
        carried = carried + jnp.exp(levels[r] - top) * parts[r][0]
    high = carried.astype(BF)
    gain = gain_ref[...].astype(F32)
    for r in (2, 1, 3, 0):
        for side, out in ((c, outs[r]), (1 - c, outs[4 + r])):
            group = side * 4 + lax.rem(x + r, 4)
            rows = pl.ds(pl.multiple_of(group * 128, 128), 128)
            line = jnp.broadcast_to(a_ref[1, pl.ds(group, 1), :], (128, 128))
            left = jnp.transpose(line)
            inner = jnp.concatenate([left, left], axis=1)
            row_max = jnp.maximum(inner, top)
            outer = jnp.dot(q_ref[rows, :], high, preferred_element_type=F32)
            memory = jnp.exp(inner - row_max) * num_ref[rows, :] + jnp.exp(top - row_max) * outer
            memory = memory * (DK**-0.5)
            mean = jnp.sum(memory * memory, axis=1, keepdims=True) * (1.0 / DV)
            normal = memory * lax.rsqrt(mean + EPSILON)
            opened = jax.nn.sigmoid(o_ref[rows, :].astype(F32))
            out[:, 0:256] = (normal * gain * opened).astype(BF)
            out[:, 256:512] = res_ref[rows, :]


def stream_body(*refs):
    keeps, others, own_w, other_w = refs[0:4], refs[4:8], refs[8:12], refs[12:16]
    out_ref, scratch = refs[16:18]
    x = lax.axis_index("x")
    c = lax.axis_index("c")
    for r in range(4):
        chip = lax.rem(x - r + 4, 4)
        scratch[chip * 2 + c] = keeps[r][:, 256:512]
        scratch[chip * 2 + 1 - c] = others[r][:, 256:512]

    def columns(n, carry):
        cols = pl.ds(pl.multiple_of(512 * n, 512), 512)
        total = jnp.concatenate(
            [scratch[2 * n].astype(F32), scratch[2 * n + 1].astype(F32)], axis=1
        )
        for r in range(4):
            total = total + jnp.dot(
                keeps[r][:, 0:256], own_w[r][:, cols], preferred_element_type=F32
            )
            total = total + jnp.dot(
                others[r][:, 0:256], other_w[r][:, cols], preferred_element_type=F32
            )
        out_ref[:, cols] = total.astype(BF)
        return carry

    lax.fori_loop(0, 4, columns, 0)


def norm_body(s0, s1, s2, s3, gain_ref, out_a, out_b, own_a, own_b, blocks):
    x = lax.axis_index("x")
    for r, s in enumerate((s0, s1, s2, s3)):
        blocks[lax.rem(x - r + 4, 4)] = s[...]
    gain = gain_ref[...].astype(F32)
    cols = pl.ds(pl.multiple_of(x * 512, 512), 512)
    for first, out, own in ((0, out_a, own_a), (2, out_b, own_b)):

        def one_block(k, carry, first=first, out=out, own=own):
            rows = pl.ds(pl.multiple_of(128 * k, 128), 128)
            wide = blocks[first + k].astype(F32)
            square = jnp.sum(wide * wide, axis=1, keepdims=True)
            scale = lax.rsqrt(square * (1.0 / 2048) + EPSILON)
            out[rows, :] = (wide * scale * gain).astype(BF)
            own[rows, :] = blocks[first + k, :, cols]
            return carry

        lax.fori_loop(0, 2, one_block, 0)


def feed_ordered(n_ref, weights, hidden, pieces, wait, outs):
    x = lax.axis_index("x")

    def open_side(side, carry):
        both = jnp.zeros((PART, 2 * FFD), F32)
        for k in range(2):
            wait(side, k)
            both = both + jnp.dot(
                n_ref[:, 1024 * k : 1024 * (k + 1)],
                weights[side, 16 * k : 16 * (k + 1), 0:64, :].reshape(1024, 2 * FFD),
                preferred_element_type=F32,
            )
        gate, up = both[:, 0:FFD], both[:, FFD : 2 * FFD]
        value = (gate * jax.nn.sigmoid(gate) * up).astype(BF)
        blank = jnp.zeros((PART, 64), BF)
        hidden[side, 0] = jnp.concatenate([value, blank], axis=1)
        hidden[side, 1] = jnp.concatenate([blank, value], axis=1)
        return carry

    lax.fori_loop(0, 2, open_side, 0)
    for side in range(2):
        wait(side, 2)
    source = lax.broadcasted_iota(jnp.int32, (HALF, HALF), 0)
    target = lax.broadcasted_iota(jnp.int32, (HALF, HALF), 1)
    wanted = ((target >> 5) & 1) * 256 + (target >> 6) * 32 + (target & 31)
    order_back = jnp.where(source == wanted, 1.0, 0.0).astype(BF)
    for r in (1, 3, 2, 0):
        begin = lax.rem(x + r, 4) * 8

        def one_group(group, carry, begin=begin):
            lanes = pl.ds(pl.multiple_of(640 * group, 128), 768)
            total = jnp.zeros((PART, 256), F32)
            for side in range(2):
                block = weights[side, pl.ds(begin, 8), 64:96, lanes].reshape(256, 768)
                total = total + lax.dot_general(
                    hidden[side, group], block, (((1,), (1,)), ((), ())),
                    preferred_element_type=F32,
                )
            pieces[group] = total.astype(BF)
            return carry

        lax.fori_loop(0, 2, one_group, 0)
        mixed_order = jnp.concatenate([pieces[0], pieces[1]], axis=1)
        outs[r][...] = jnp.dot(
            mixed_order, order_back, preferred_element_type=F32
        ).astype(BF)


PIECES = (((0, 16), (0, 64)), ((16, 16), (0, 64)), ((0, 32), (64, 32)))


def feed_a_body(n_ref, w_ref, o0, o1, o2, o3, weights, hidden, pieces, sems):
    def copy(side, part):
        (first, count), (top, height) = PIECES[part]
        return pltpu.make_async_copy(
            w_ref.at[pl.ds(first, count), side, pl.ds(top, height), :],
            weights.at[side, pl.ds(first, count), pl.ds(top, height), :],
            sems.at[side, part],
        )

    for side, part in ((0, 0), (0, 1), (1, 0), (1, 1), (0, 2), (1, 2)):
        copy(side, part).start()
    feed_ordered(
        n_ref, weights, hidden, pieces, lambda side, part: copy(side, part).wait(), (o0, o1, o2, o3)
    )


def feed_b_body(n_ref, weights, o0, o1, o2, o3, hidden, pieces):
    feed_ordered(n_ref, weights, hidden, pieces, lambda side, part: None, (o0, o1, o2, o3))


def mixed_halves(stream_ref, parts):
    c = lax.axis_index("c")
    total = sum(p[...].astype(F32) for p in parts)
    mixed = (stream_ref[...].astype(F32) + 0.5 * total).astype(BF)
    left, right = mixed[:, 0:256], mixed[:, 256:512]
    return jnp.where(c == 0, left, right), jnp.where(c == 0, right, left)


def mix_a_body(stream_ref, p0, p1, p2, p3, mine_ref, send_ref):
    mine_ref[...], send_ref[...] = mixed_halves(stream_ref, (p0, p1, p2, p3))


def mix_b_body(stream_ref, p0, p1, p2, p3, mine_a, theirs_a, whole_ref, send_ref):
    c = lax.axis_index("c")
    mine, send_ref[...] = mixed_halves(stream_ref, (p0, p1, p2, p3))
    own = pl.multiple_of(c * HALF, PART)
    other = pl.multiple_of((1 - c) * HALF, PART)
    whole_ref[pl.ds(own, PART), :] = mine_a[...]
    whole_ref[pl.ds(own + PART, PART), :] = mine
    whole_ref[pl.ds(other, PART), :] = theirs_a[...]
    whole_ref[pl.ds(other + PART, PART), :] = mine


def shift(array, axis, count, by):
    return lax.ppermute(array, axis, [(i, (i + by) % count) for i in range(count)])


def column(array, steps):
    pairs = []
    for y in range(4):
        for z in range(8 - steps[y]):
            pairs.append((4 * z + y, 4 * (z + steps[y]) + y))
    return lax.ppermute(array, SP, pairs)


def swap(array):
    return lax.ppermute(array, "c", [(0, 1), (1, 0)])


def cross(array, by):
    pairs = []
    for i in range(4):
        for j in range(2):
            pairs.append((2 * i + j, 2 * ((i + by) % 4) + 1 - j))
    return lax.ppermute(array, TP, pairs)


def spread(array, axis):
    return [array] + [shift(array, axis, 4, r) for r in (1, 2, 3)]


def layer(
    queries,
    cell_key_rows,
    cell_value_rows,
    output_gate_logits,
    input_gate_logits,
    forget_gate_logits,
    forget_extra_term,
    residual,
    head_norm_gain,
    cell_output_weight,
    feedforward_norm_gain,
    gate_projection_weight,
    up_projection_weight,
    down_projection_weight,
):
    c = lax.axis_index("c")

    own_out = spread(cell_output_weight, "x")
    other_out = [swap(rows) for rows in own_out]

    message, levels = call(
        summary_body,
        (shape((MSG, DV)), shape((2, 8, 128), F32)),
        (cell_key_rows, cell_value_rows, input_gate_logits, forget_gate_logits, forget_extra_term),
        vmem=60,
    )
    near = spread(message, "y")[1:]

    turned = down_projection_weight.T
    shard = jnp.concatenate(
        [
            jnp.concatenate([gate_projection_weight, up_projection_weight], axis=1),
            jnp.concatenate([turned[0:32], turned[32:64]], axis=1),
        ],
        axis=0,
    )
    weights = lax.all_gather(shard, ("z", "y", "c")).reshape(32, 2, 96, 2 * FFD)

    numerator = call(
        inside_body,
        shape((ROWS, DV), F32),
        (queries, cell_key_rows, cell_value_rows, levels),
        flops=2000000000,
        vmem=60,
    )
    plane, prefix = call(
        plane_body, (shape((MSG, DV)), shape((MSG, DV), F32)), (message, *near), in_specs=[VMEM] * 4
    )
    joined = call(
        join_body,
        shape((MSG, DV)),
        (column(plane, (1, 3, 5, 7)), column(plane, (2, 4, 6, 8))),
        in_specs=[VMEM] * 2,
    )
    gated = call(
        gated_body,
        tuple(shape((128, 512)) for _ in range(8)),
        (*spread(joined, "y"), prefix, numerator, queries, levels,
         output_gate_logits, head_norm_gain.reshape(1, DV), residual),
        in_specs=[VMEM] * 11,
        vmem=60,
    )
    keeps = [gated[0]] + [shift(gated[r], "x", 4, r) for r in (1, 2, 3)]
    others = [cross(gated[4 + r], r) for r in range(4)]
    stream = call(
        stream_body,
        shape((128, 2048)),
        (*keeps, *others, *own_out, *other_out),
        in_specs=[VMEM] * 16,
        scratch=(pltpu.VMEM((8, 128, 256), BF),),
        vmem=20,
    )
    streams = spread(stream, "x")
    normed_a, normed_b, own_a, own_b = call(
        norm_body,
        (shape((PART, 2048)), shape((PART, 2048)), shape((PART, HALF)), shape((PART, HALF))),
        (*streams, feedforward_norm_gain.reshape(1, 2048)),
        in_specs=[VMEM] * 5,
        scratch=(pltpu.VMEM((4, 128, 2048), BF),),
    )

    def exchanged(parts):
        return [parts[0]] + [shift(parts[r], "x", 4, r) for r in (1, 2, 3)]

    *parts_a, resident = call(
        feed_a_body,
        tuple(shape((PART, HALF)) for _ in range(4)) + (shape((2, 32, 96, 2 * FFD)),),
        (normed_a, weights),
        in_specs=[VMEM, ANY],
        scratch=(pltpu.VMEM((2, 2, PART, 768), BF), pltpu.VMEM((2, PART, 256), BF), pltpu.SemaphoreType.DMA((2, 3))),
        flops=4500000000,
        vmem=FEED_VMEM,
    )
    parts_b = call(
        feed_b_body,
        tuple(shape((PART, HALF)) for _ in range(4)),
        (normed_b, resident),
        scratch=(pltpu.VMEM((2, 2, PART, 768), BF), pltpu.VMEM((2, PART, 256), BF)),
        flops=4500000000,
        vmem=FEED_VMEM,
    )
    arrived_a = exchanged(parts_a)
    arrived_b = exchanged(parts_b)
    mine_a, theirs_a = call(
        mix_a_body,
        (shape((PART, 256)), shape((PART, 256))),
        (own_a, *arrived_a),
        in_specs=[VMEM] * 5,
    )
    whole, theirs_b = call(
        mix_b_body,
        (shape((ROWS, 256)), shape((PART, 256))),
        (own_b, *arrived_b, mine_a, swap(theirs_a)),
        in_specs=[VMEM] * 7,
    )
    return lax.dynamic_update_slice(whole, swap(theirs_b), ((1 - c) * HALF + PART, jnp.int32(0)))


def solution(mesh):
    torus = Mesh(mesh.devices.reshape(8, 4, 4, 2), ("z", "y", "x", "c"))
    in_specs = (
        P(SP, TP),
        P(SP, TP),
        P(SP, TP),
        P(SP, TP),
        P(TP, SP),
        P(TP, SP),
        P(TP, SP),
        P(SP, TP),
        P(TP),
        P(TP, None),
        P(),
        P(SP, TP),
        P(SP, TP),
        P(TP, SP),
    )
    out_specs = P(SP, TP)
    return jax.shard_map(layer, mesh=torus, in_specs=in_specs, out_specs=out_specs, check_vma=False)
```

```python
import functools

import jax
import jax.numpy as jnp
from jax import lax
from jax.experimental import pallas as pl
from jax.experimental.pallas import tpu as pltpu
from jax.sharding import Mesh
from jax.sharding import PartitionSpec as P


SP = ("z", "y")
TP = ("x", "c")
BF = jnp.bfloat16
F32 = jnp.float32
LOWEST = -1e30
EPSILON = 1e-06
ROWS = 1024
HALF = 512
PART = 256
DK = 128
DV = 256
MSG = 144
FFD = 704
FEED_VMEM = 20

VMEM = pl.BlockSpec(memory_space=pltpu.VMEM)
SMEM = pl.BlockSpec(memory_space=pltpu.SMEM)
ANY = pl.BlockSpec(memory_space=pltpu.HBM)


def call(body, outs, ins, scratch=(), flops=1000000, in_specs=None, vmem=12):
    return pl.pallas_call(
        body,
        out_shape=outs,
        in_specs=in_specs or [VMEM] * len(ins),
        out_specs=jax.tree.map(lambda _: VMEM, outs),
        scratch_shapes=list(scratch),
        cost_estimate=pl.CostEstimate(flops=flops, bytes_accessed=1000000, transcendentals=0),
        compiler_params=pltpu.CompilerParams(vmem_limit_bytes=vmem * 1024 * 1024),
    )(*ins)


def shape(dims, dtype=BF):
    return jax.ShapeDtypeStruct(dims, dtype)


def scan_rows(values, combine, fill):
    lane = lax.broadcasted_iota(jnp.int32, (8, 128), 1)
    row = lax.broadcasted_iota(jnp.int32, (8, 128), 0)
    for step in (1, 2, 4, 8, 16, 32, 64):
        moved = pltpu.roll(values, step, 1)
        values = combine(values, jnp.where(lane >= step, moved, fill))
    last = jnp.broadcast_to(values[:, 127:128], (8, 128))
    before = jnp.where(row >= 1, pltpu.roll(last, 1, 0), fill)
    for step in (1, 2, 4):
        moved = pltpu.roll(before, step, 0)
        before = combine(before, jnp.where(row >= step, moved, fill))
    return combine(values, before)


def eight_rows(ref):
    wide = ref[...].astype(F32)
    return jnp.concatenate([wide[:, 128 * k : 128 * (k + 1)] for k in range(8)], axis=0)


def as_column(values, k):
    return jnp.transpose(jnp.broadcast_to(values[k : k + 1, :], (128, 128)))


def split3(value):
    high = value.astype(BF).astype(F32)
    middle = (value - high).astype(BF).astype(F32)
    return high, middle, value - high - middle


def scalar_tile(top, total, width=256):
    row = lax.broadcasted_iota(jnp.int32, (16, width), 0)
    tile = jnp.zeros((16, width), F32)
    for k, part in enumerate(split3(top) + split3(total)):
        tile = jnp.where(row == k, jnp.broadcast_to(part, (16, width)), tile)
    return tile.astype(BF)


def read_message(ref):
    tile = ref[DK:MSG, :].astype(F32)
    top = tile[0:1] + tile[1:2] + tile[2:3]
    total = tile[3:4] + tile[4:5] + tile[5:6]
    return ref[0:DK, :].astype(F32), top, total


def summary_body(k_ref, v_ref, ig_ref, fg_ref, fe_ref, msg_ref, a_ref):
    gate = eight_rows(ig_ref)
    forget = eight_rows(fg_ref)
    extra = eight_rows(fe_ref)
    small = jnp.exp(-jnp.abs(forget))
    series = small * (1.0 - small * (0.5 - small * (1 / 3 - small * (0.25 - small * 0.2))))
    log_one = jnp.where(small < 0.03, series, jnp.log(1.0 + small))
    log_forget = jnp.minimum(forget, 0.0) - log_one + extra
    running = scan_rows(log_forget, jnp.add, 0.0)
    level = gate - running
    highest = scan_rows(level, jnp.maximum, LOWEST)
    a_ref[0] = level
    a_ref[1] = highest
    final = jnp.broadcast_to(highest[7:8, 127:128], (8, 128))
    weight = jnp.exp(level - final)
    total = jnp.zeros((DK, DV), F32)
    for b in range(8):
        rows = slice(128 * b, 128 * (b + 1))
        scaled = (k_ref[rows, :].astype(F32) * as_column(weight, b)).astype(BF)
        total = total + lax.dot_general(
            scaled, v_ref[rows, :], (((0,), (0,)), ((), ())), preferred_element_type=F32
        )
    msg_ref[0:DK, :] = total.astype(BF)
    all_forget = running[7:8, 127:128]
    msg_ref[DK:MSG, :] = scalar_tile(highest[7:8, 127:128] + all_forget, all_forget)


def inside_body(q_ref, k_ref, v_ref, a_ref, num_ref):
    level = a_ref[0]
    highest = a_ref[1]
    t = lax.broadcasted_iota(jnp.int32, (256, 256), 0)
    s = lax.broadcasted_iota(jnp.int32, (256, 256), 1)
    causal = t >= s
    for i in range(4):
        left = jnp.concatenate([as_column(highest, 2 * i), as_column(highest, 2 * i + 1)], axis=0)
        column = jnp.concatenate([left, left], axis=1)
        query = q_ref[256 * i : 256 * (i + 1), :]
        total = jnp.zeros((256, DV), F32)
        for j in range(i + 1):
            rows = slice(256 * j, 256 * (j + 1))
            line = jnp.concatenate([level[2 * j : 2 * j + 1], level[2 * j + 1 : 2 * j + 2]], axis=1)
            score = lax.dot_general(
                query, k_ref[rows, :], (((1,), (1,)), ((), ())), preferred_element_type=F32
            )
            weight = jnp.exp(line - column)
            if i == j:
                weight = jnp.where(causal, weight, 0.0)
            total = total + jnp.dot(
                (score * weight).astype(BF), v_ref[rows, :], preferred_element_type=F32
            )
        num_ref[256 * i : 256 * (i + 1), :] = total


def plane_body(m0, m1, m2, m3, plane_ref, prefix_ref):
    y = lax.axis_index("y")
    parts = [read_message(m) for m in (m0, m1, m2, m3)]
    place = [lax.rem(y - r + 4, 4) for r in range(4)]
    levels, befores = [], []
    total_all = jnp.zeros((1, DV), F32)
    total_before = jnp.zeros((1, DV), F32)
    for r in range(4):
        level = parts[r][1]
        before = parts[r][1]
        for w in range(4):
            if w != r:
                later = place[w] > place[r]
                level = level + jnp.where(later, parts[w][2], 0.0)
                before = before + jnp.where(later & (place[w] < y), parts[w][2], 0.0)
        levels.append(level)
        befores.append(jnp.where(place[r] < y, before, LOWEST))
        total_all = total_all + parts[r][2]
        total_before = total_before + jnp.where(place[r] < y, parts[r][2], 0.0)
    top = functools.reduce(jnp.maximum, levels)
    top_before = functools.reduce(jnp.maximum, befores)
    whole = jnp.zeros((DK, DV), F32)
    early = jnp.zeros((DK, DV), F32)
    for r in range(4):
        whole = whole + jnp.exp(levels[r] - top) * parts[r][0]
        share = jnp.where(place[r] < y, jnp.exp(befores[r] - top_before), 0.0)
        early = early + share * parts[r][0]
    plane_ref[0:DK, :] = whole.astype(BF)
    plane_ref[DK:MSG, :] = scalar_tile(top, total_all)
    prefix_ref[0:DK, :] = early
    prefix_ref[DK : DK + 8, :] = jnp.broadcast_to(top_before, (8, DV))
    prefix_ref[DK + 8 : DK + 16, :] = jnp.broadcast_to(total_before, (8, DV))


def join_body(near_ref, far_ref, out_ref):
    z, y = lax.axis_index("z"), lax.axis_index("y")
    state_near, top_near, total_near = read_message(near_ref)
    state_far, top_far, total_far = read_message(far_ref)
    has_near = z >= 2 * y + 1
    has_far = (z >= 2 * y + 2) & (y < 3)
    top_near = jnp.where(has_near, top_near, LOWEST)
    total_near = jnp.where(has_near, total_near, 0.0)
    moved = jnp.where(has_far, top_far + total_near, LOWEST)
    total_far = jnp.where(has_far, total_far, 0.0)
    top = jnp.maximum(top_near, moved)
    share_near = jnp.where(has_near, jnp.exp(top_near - top), 0.0)
    share_far = jnp.where(has_far, jnp.exp(moved - top), 0.0)
    out_ref[0:DK, :] = (share_near * state_near + share_far * state_far).astype(BF)
    out_ref[DK:MSG, :] = scalar_tile(top, total_near + total_far)


def gated_body(
    m0, m1, m2, m3, prefix_ref, num_ref, q_ref, a_ref, o_ref, gain_ref, res_ref, *outs
):
    y = lax.axis_index("y")
    x = lax.axis_index("x")
    c = lax.axis_index("c")
    top_before = prefix_ref[DK : DK + 1, :]
    parts = [read_message(m) for m in (m0, m1, m2, m3)]
    place = [lax.rem(y - r + 4, 4) for r in range(4)]
    levels = []
    for r in range(4):
        level = parts[r][1] + prefix_ref[DK + 8 : DK + 9, :]
        for w in range(4):
            if w != r:
                level = level + jnp.where(place[w] < place[r], parts[w][2], 0.0)
        levels.append(level)
    top = functools.reduce(jnp.maximum, levels, top_before)
    carried = jnp.exp(top_before - top) * prefix_ref[0:DK, :]
    for r in range(4):
        carried = carried + jnp.exp(levels[r] - top) * parts[r][0]
    high = carried.astype(BF)
    gain = gain_ref[...].astype(F32)
    for r in (2, 1, 3, 0):
        for side, out in ((c, outs[r]), (1 - c, outs[4 + r])):
            group = side * 4 + lax.rem(x + r, 4)
            rows = pl.ds(pl.multiple_of(group * 128, 128), 128)
            line = jnp.broadcast_to(a_ref[1, pl.ds(group, 1), :], (128, 128))
            left = jnp.transpose(line)
            inner = jnp.concatenate([left, left], axis=1)
            row_max = jnp.maximum(inner, top)
            outer = jnp.dot(q_ref[rows, :], high, preferred_element_type=F32)
            memory = jnp.exp(inner - row_max) * num_ref[rows, :] + jnp.exp(top - row_max) * outer
            memory = memory * (DK**-0.5)
            mean = jnp.sum(memory * memory, axis=1, keepdims=True) * (1.0 / DV)
            normal = memory * lax.rsqrt(mean + EPSILON)
            opened = jax.nn.sigmoid(o_ref[rows, :].astype(F32))
            out[:, 0:256] = (normal * gain * opened).astype(BF)
            out[:, 256:512] = res_ref[rows, :]


def stream_body(*refs):
    keeps, others, own_w, other_w = refs[0:4], refs[4:8], refs[8:12], refs[12:16]
    out_ref, scratch = refs[16:18]
    x = lax.axis_index("x")
    c = lax.axis_index("c")
    for r in range(4):
        chip = lax.rem(x - r + 4, 4)
        scratch[chip * 2 + c] = keeps[r][:, 256:512]
        scratch[chip * 2 + 1 - c] = others[r][:, 256:512]

    def columns(n, carry):
        cols = pl.ds(pl.multiple_of(512 * n, 512), 512)
        total = jnp.concatenate(
            [scratch[2 * n].astype(F32), scratch[2 * n + 1].astype(F32)], axis=1
        )
        for r in range(4):
            total = total + jnp.dot(
                keeps[r][:, 0:256], own_w[r][:, cols], preferred_element_type=F32
            )
            total = total + jnp.dot(
                others[r][:, 0:256], other_w[r][:, cols], preferred_element_type=F32
            )
        out_ref[:, cols] = total.astype(BF)
        return carry

    lax.fori_loop(0, 4, columns, 0)


def norm_body(s0, s1, s2, s3, gain_ref, out_a, out_b, own_a, own_b, blocks):
    x = lax.axis_index("x")
    for r, s in enumerate((s0, s1, s2, s3)):
        blocks[lax.rem(x - r + 4, 4)] = s[...]
    gain = gain_ref[...].astype(F32)
    cols = pl.ds(pl.multiple_of(x * 512, 512), 512)
    for first, out, own in ((0, out_a, own_a), (2, out_b, own_b)):

        def one_block(k, carry, first=first, out=out, own=own):
            rows = pl.ds(pl.multiple_of(128 * k, 128), 128)
            wide = blocks[first + k].astype(F32)
            square = jnp.sum(wide * wide, axis=1, keepdims=True)
            scale = lax.rsqrt(square * (1.0 / 2048) + EPSILON)
            out[rows, :] = (wide * scale * gain).astype(BF)
            own[rows, :] = blocks[first + k, :, cols]
            return carry

        lax.fori_loop(0, 2, one_block, 0)


def feed_ordered(n_ref, gates, downs, hidden, wait, outs):
    x = lax.axis_index("x")

    def open_side(side, carry):
        wait(side, 0)
        both = jnp.dot(
            n_ref[...], gates[side].reshape(2048, 2 * FFD), preferred_element_type=F32
        )
        gate, up = both[:, 0:FFD], both[:, FFD : 2 * FFD]
        value = (gate * jax.nn.sigmoid(gate) * up).astype(BF)
        hidden[side] = jnp.concatenate([value, jnp.zeros((PART, 64), BF)], axis=1)
        wait(side, 1)
        return carry

    lax.fori_loop(0, 2, open_side, 0)
    for r in (1, 3, 2, 0):
        begin = lax.rem(x + r, 4) * 8
        total = jnp.zeros((PART, HALF), F32)
        for side in range(2):
            block = downs[side, pl.ds(begin, 8)].reshape(512, 768)
            total = total + lax.dot_general(
                hidden[side], block, (((1,), (1,)), ((), ())), preferred_element_type=F32
            )
        outs[r][...] = total.astype(BF)


def feed_a_body(n_ref, w_ref, o0, o1, o2, o3, gates, downs, hidden, sems):
    def copies(side, part):
        if part == 0:
            pairs = ((w_ref.at[:, side, pl.ds(0, 64), :], gates.at[side]),)
        else:
            pairs = tuple(
                (
                    w_ref.at[:, side, pl.ds(64, 32), pl.ds(640 * group, 768)],
                    downs.at[side, :, pl.ds(32 * group, 32), :],
                )
                for group in range(2)
            )
        return [
            pltpu.make_async_copy(source, target, sems.at[side, part + n])
            for n, (source, target) in enumerate(pairs)
        ]

    for side in range(2):
        for part in range(2):
            for copy in copies(side, part):
                copy.start()

    def wait(side, part):
        for copy in copies(side, part):
            copy.wait()
        if part == 1:
            raw = downs[side, :, 32:64, :].reshape(1024, 768)
            moved = jnp.concatenate([raw[:, 64:768], jnp.zeros((1024, 64), BF)], axis=1)
            downs[side, :, 32:64, :] = moved.reshape(32, 32, 768)

    feed_ordered(n_ref, gates, downs, hidden, wait, (o0, o1, o2, o3))


def feed_b_body(n_ref, gates, downs, o0, o1, o2, o3, hidden):
    feed_ordered(n_ref, gates, downs, hidden, lambda side, part: None, (o0, o1, o2, o3))


def mixed_halves(stream_ref, parts):
    c = lax.axis_index("c")
    total = sum(p[...].astype(F32) for p in parts)
    mixed = (stream_ref[...].astype(F32) + 0.5 * total).astype(BF)
    left, right = mixed[:, 0:256], mixed[:, 256:512]
    return jnp.where(c == 0, left, right), jnp.where(c == 0, right, left)


def mix_a_body(stream_ref, p0, p1, p2, p3, mine_ref, send_ref):
    mine_ref[...], send_ref[...] = mixed_halves(stream_ref, (p0, p1, p2, p3))


def mix_b_body(stream_ref, p0, p1, p2, p3, mine_a, theirs_a, whole_ref, send_ref):
    c = lax.axis_index("c")
    mine, send_ref[...] = mixed_halves(stream_ref, (p0, p1, p2, p3))
    own = pl.multiple_of(c * HALF, PART)
    other = pl.multiple_of((1 - c) * HALF, PART)
    whole_ref[pl.ds(own, PART), :] = mine_a[...]
    whole_ref[pl.ds(own + PART, PART), :] = mine
    whole_ref[pl.ds(other, PART), :] = theirs_a[...]
    whole_ref[pl.ds(other + PART, PART), :] = mine


def shift(array, axis, count, by):
    return lax.ppermute(array, axis, [(i, (i + by) % count) for i in range(count)])


def column(array, steps):
    pairs = []
    for y in range(4):
        for z in range(8 - steps[y]):
            pairs.append((4 * z + y, 4 * (z + steps[y]) + y))
    return lax.ppermute(array, SP, pairs)


def swap(array):
    return lax.ppermute(array, "c", [(0, 1), (1, 0)])


def cross(array, by):
    pairs = []
    for i in range(4):
        for j in range(2):
            pairs.append((2 * i + j, 2 * ((i + by) % 4) + 1 - j))
    return lax.ppermute(array, TP, pairs)


def spread(array, axis):
    return [array] + [shift(array, axis, 4, r) for r in (1, 2, 3)]


def layer(
    queries,
    cell_key_rows,
    cell_value_rows,
    output_gate_logits,
    input_gate_logits,
    forget_gate_logits,
    forget_extra_term,
    residual,
    head_norm_gain,
    cell_output_weight,
    feedforward_norm_gain,
    gate_projection_weight,
    up_projection_weight,
    down_projection_weight,
):
    c = lax.axis_index("c")

    own_out = spread(cell_output_weight, "x")
    other_out = [swap(rows) for rows in own_out]

    message, levels = call(
        summary_body,
        (shape((MSG, DV)), shape((2, 8, 128), F32)),
        (cell_key_rows, cell_value_rows, input_gate_logits, forget_gate_logits, forget_extra_term),
        vmem=60,
    )
    near = spread(message, "y")[1:]

    turned = down_projection_weight.T
    shard = jnp.concatenate(
        [
            jnp.concatenate([gate_projection_weight, up_projection_weight], axis=1),
            jnp.concatenate([turned[0:32], turned[32:64]], axis=1),
        ],
        axis=0,
    )
    weights = lax.all_gather(shard, ("z", "y", "c")).reshape(32, 2, 96, 2 * FFD)

    numerator = call(
        inside_body,
        shape((ROWS, DV), F32),
        (queries, cell_key_rows, cell_value_rows, levels),
        flops=2000000000,
        vmem=60,
    )
    plane, prefix = call(
        plane_body, (shape((MSG, DV)), shape((MSG, DV), F32)), (message, *near), in_specs=[VMEM] * 4
    )
    joined = call(
        join_body,
        shape((MSG, DV)),
        (column(plane, (1, 3, 5, 7)), column(plane, (2, 4, 6, 8))),
        in_specs=[VMEM] * 2,
    )
    gated = call(
        gated_body,
        tuple(shape((128, 512)) for _ in range(8)),
        (*spread(joined, "y"), prefix, numerator, queries, levels,
         output_gate_logits, head_norm_gain.reshape(1, DV), residual),
        in_specs=[VMEM] * 11,
        vmem=60,
    )
    keeps = [gated[0]] + [shift(gated[r], "x", 4, r) for r in (1, 2, 3)]
    others = [cross(gated[4 + r], r) for r in range(4)]
    stream = call(
        stream_body,
        shape((128, 2048)),
        (*keeps, *others, *own_out, *other_out),
        in_specs=[VMEM] * 16,
        scratch=(pltpu.VMEM((8, 128, 256), BF),),
        vmem=20,
    )
    streams = spread(stream, "x")
    normed_a, normed_b, own_a, own_b = call(
        norm_body,
        (shape((PART, 2048)), shape((PART, 2048)), shape((PART, HALF)), shape((PART, HALF))),
        (*streams, feedforward_norm_gain.reshape(1, 2048)),
        in_specs=[VMEM] * 5,
        scratch=(pltpu.VMEM((4, 128, 2048), BF),),
    )

    def exchanged(parts):
        return [parts[0]] + [shift(parts[r], "x", 4, r) for r in (1, 2, 3)]

    *parts_a, gates, downs = call(
        feed_a_body,
        tuple(shape((PART, HALF)) for _ in range(4))
        + (shape((2, 32, 64, 2 * FFD)), shape((2, 32, 64, 768))),
        (normed_a, weights),
        in_specs=[VMEM, ANY],
        scratch=(pltpu.VMEM((2, PART, 768), BF), pltpu.SemaphoreType.DMA((2, 3))),
        flops=4500000000,
        vmem=FEED_VMEM,
    )
    parts_b = call(
        feed_b_body,
        tuple(shape((PART, HALF)) for _ in range(4)),
        (normed_b, gates, downs),
        scratch=(pltpu.VMEM((2, PART, 768), BF),),
        flops=4500000000,
        vmem=FEED_VMEM,
    )
    arrived_a = exchanged(parts_a)
    arrived_b = exchanged(parts_b)
    mine_a, theirs_a = call(
        mix_a_body,
        (shape((PART, 256)), shape((PART, 256))),
        (own_a, *arrived_a),
        in_specs=[VMEM] * 5,
    )
    whole, theirs_b = call(
        mix_b_body,
        (shape((ROWS, 256)), shape((PART, 256))),
        (own_b, *arrived_b, mine_a, swap(theirs_a)),
        in_specs=[VMEM] * 7,
    )
    return lax.dynamic_update_slice(whole, swap(theirs_b), ((1 - c) * HALF + PART, jnp.int32(0)))


def solution(mesh):
    torus = Mesh(mesh.devices.reshape(8, 4, 4, 2), ("z", "y", "x", "c"))
    in_specs = (
        P(SP, TP),
        P(SP, TP),
        P(SP, TP),
        P(SP, TP),
        P(TP, SP),
        P(TP, SP),
        P(TP, SP),
        P(SP, TP),
        P(TP),
        P(TP, None),
        P(),
        P(SP, TP),
        P(SP, TP),
        P(TP, SP),
    )
    out_specs = P(SP, TP)
    return jax.shard_map(layer, mesh=torus, in_specs=in_specs, out_specs=out_specs, check_vma=False)
```
